32 devices in a mesh: ep: 16 (over z, y, x), tp: 2 (over core).
Axes of the slice: x: 2, y: 2, z: 4, core: 2. Of those that a mesh axis runs over, the one named last changes fastest.
Arguments:
- tokens: bfloat16 [8192, 2048], P(('ep', 'tp')), may hold values from -6 to 6
- norm_gain: float32 [2048], replicated, may hold values from 0.1 to 1.9
- norm_bias: float32 [2048], replicated, may hold values from -3 to 3
- gate_weight: bfloat16 [16, 2048, 1024], P('ep', None, 'tp'), may hold values from -0.125 to 0.125
- up_weight: bfloat16 [16, 2048, 1024], P('ep', None, 'tp'), may hold values from -0.125 to 0.125
- down_weight: bfloat16 [16, 1024, 2048], P('ep', 'tp'), may hold values from -0.1875 to 0.1875
- expert_ids: int32 [8192, 2], P(('ep', 'tp')), may hold values from 0 to 15, all different within a row; in each aligned block of 256 rows (0 to 255, 256 to 511, ...) at most 64 rows name the same one
- route_weights: float32 [8192, 2], P(('ep', 'tp')), may hold values from 0.2 to 1
Outputs:
- mixed: bfloat16 [8192, 2048], P(('ep', 'tp'))
The draws below stay inside these ranges and needn't reach their ends.
Inputs may be any that keep to these rules, and one draw needn't show every extreme that they name: `expert_ids`: a token's 2 experts differ; in the tokens of one device (aligned blocks of 256 rows) no expert is named by more than 64 entries, a bound that some block reaches.
All inputs are finite; a program needn't handle non-finite values.
Results may differ from the reference program's by a relative error of at most 0.0071.
Values may be sent and summed in bfloat16 or wider, within the bound.
A program may use at most 128 MiB of HBM per device.

```python
import math
import jax
import jax.numpy as jnp
import numpy as np
from jax import lax

D = 2048
FFE = 1024
TOPK = 2
TOK_DEV = 256
EXPERTS = 16
CAP = 64
TOKENS = 8192


def block_scale(key, dims, cuts, least, high):
    def one(dim, shards_of):
        draws = jax.random.uniform(jax.random.fold_in(jax.random.fold_in(key, 6), dim), (shards_of,), jnp.float32, least / len(cuts), high / len(cuts))
        return jnp.repeat(jnp.exp(draws), dims[dim] // shards_of).reshape((-1,) + (1,) * (len(dims) - dim - 1))

    level = one(*cuts[0])
    for cut in cuts[1:]:
        level = level * one(*cut)
    return level


def assign_block(stream_key, own, number, rows, number_of, top, limit, skew):
    ranking = jax.random.permutation(stream_key, number_of)
    heavy_load, common = shares(number_of, rows * top, limit, skew, True), shares(number_of, rows * top, limit, skew, False)
    places = jnp.arange(number_of)

    def named(tallies, offset_by):
        used = int((tallies > 0).sum())
        fixed = max(1, used // 4)
        moved = fixed + (places - fixed + offset_by * (used - fixed)) % max(1, number_of - fixed)
        return jnp.zeros((number_of,), jnp.int32).at[ranking[jnp.where(places < fixed, places, moved)]].set(jnp.asarray(tallies, jnp.int32))

    tallies = jnp.where(number % 4 == 0, named(heavy_load, number // 4), named(common, number - number // 4 - 1))
    mixed = jax.random.permutation(jax.random.fold_in(own, 3), number_of)
    source_of, receiver = mixed[0:number_of // 2 * 2:2], mixed[1:number_of // 2 * 2:2]
    room = jnp.minimum(tallies[source_of] - 1, limit - tallies[receiver]) // 2
    room = jnp.where((source_of == ranking[0]) | (receiver == ranking[0]) | (tallies[receiver] == 0), 0, jnp.maximum(room, 0))
    moved = jax.random.randint(jax.random.fold_in(own, 4), (number_of // 2,), 0, 1 << 20) % (room + 1)
    tallies = tallies.at[source_of].add(-moved).at[receiver].add(moved)
    members = jnp.searchsorted(jnp.cumsum(tallies), jnp.arange(rows * top), side="right").astype(jnp.int32)
    grid = members.reshape(top, rows).T
    grid = grid[jax.random.permutation(jax.random.fold_in(own, 1), rows)]
    offset_by = jax.random.randint(jax.random.fold_in(own, 2), (rows, 1), 0, top)
    return jnp.take_along_axis(grid, (jnp.arange(top)[None, :] + offset_by) % top, axis=1)


def shares(number_of, total, bound, slope, full):
    loads = [(1 << 20) // math.isqrt(rank ** slope) + 1 for rank in range(1, number_of + 1)]
    largest = bound if full else min(bound, max(-(-total // number_of), total * loads[0] // sum(loads)))
    least = 1 if total - largest >= number_of - 1 else 0
    counts, rest = [largest] + [least] * (number_of - 1), total - largest - least * (number_of - 1)
    while rest > 0:
        candidates = [i for i in range(1, number_of) if counts[i] < largest] or [i for i in range(1, number_of) if counts[i] < bound]
        pool, left = sum([loads[i] for i in candidates]), rest
        for i in candidates:
            more = min(bound - counts[i], max(1, left * loads[i] // pool), rest)
            counts[i] = counts[i] + more
            rest = rest - more
    return np.array(counts)


def scatter_about(own_key, shape, width, bound, cuts=(), held_as=jnp.bfloat16):
    array = jax.random.normal(own_key, shape, jnp.float32) * width
    if len(cuts) > 0:
        array = block_scale(own_key, shape, cuts, -0.22, 0.18) * array
    return jnp.clip(array, min=-bound, max=bound).astype(held_as)


def setup_inputs(seed: int = 0) -> dict:
    seeds = jax.random.split(jax.random.key(seed), 9)
    tokens = scatter_about(seeds[0], (TOKENS, D), 1.0, 6.0, ((0, 32),))
    norm_gain = jnp.clip(1.0 + 0.18 * jax.random.normal(seeds[1], (D,), jnp.float32), 0.1, 1.9)
    norm_bias = scatter_about(seeds[2], (D,), 0.5, 3.0, (), jnp.float32)
    gate_weight = scatter_about(seeds[3], (EXPERTS, D, FFE), D ** -0.5, 0.125, ((0, 16), (2, 2)))
    up_weight = scatter_about(seeds[4], (EXPERTS, D, FFE), D ** -0.5, 0.125, ((0, 16), (2, 2)))
    down_weight = scatter_about(seeds[5], (EXPERTS, FFE, D), FFE ** -0.5, 0.1875, ((0, 16), (1, 2)))
    expert_ids_keys = jax.random.split(jax.random.fold_in(seeds[6], 1), TOKENS // TOK_DEV)
    expert_ids_turns = jax.random.permutation(jax.random.fold_in(seeds[6], 3), TOKENS // TOK_DEV)
    expert_ids = jax.vmap(lambda own, number: assign_block(jax.random.fold_in(seeds[6], 2), own, number, TOK_DEV, EXPERTS, TOPK, CAP, 2))(expert_ids_keys, expert_ids_turns).reshape((TOKENS, TOPK))
    route_weights = jnp.clip(0.2 + 0.8 * jax.random.uniform(seeds[7], (TOKENS, TOPK), jnp.float32) ** block_scale(seeds[7], (TOKENS, TOPK), ((0, 32),), -0.2, 0.2), 0.2, 1.0)
    return {"tokens": tokens, "norm_gain": norm_gain, "norm_bias": norm_bias, "gate_weight": gate_weight, "up_weight": up_weight, "down_weight": down_weight, "expert_ids": expert_ids, "route_weights": route_weights}


def expert_rows(rows, w_gate, w_up, w_down):
    gate = jnp.dot(rows, w_gate, preferred_element_type=jnp.float32)
    upper = jnp.dot(rows, w_up, preferred_element_type=jnp.float32)
    hidden = (jax.nn.silu(gate) * upper).astype(jnp.bfloat16)
    return jnp.dot(hidden, w_down, preferred_element_type=jnp.float32).astype(jnp.bfloat16)

def reference(tokens, norm_gain, norm_bias, gate_weight, up_weight, down_weight, expert_ids, route_weights):
    values = tokens.astype(jnp.float32)
    centre = values - lax.optimization_barrier(jnp.mean(values, axis=-1, keepdims=True))
    spread = lax.optimization_barrier(jnp.mean(centre * centre, axis=-1, keepdims=True))
    normed = (centre * lax.rsqrt(spread + 1e-05) * norm_gain + norm_bias).astype(jnp.bfloat16)
    sources = TOKENS // TOK_DEV
    blocks = expert_ids.reshape(sources, TOK_DEV * TOPK)
    onehot = (blocks[:, :, None] == jnp.arange(EXPERTS, dtype=jnp.int32)[None, None, :]).astype(jnp.int32)
    slot = lax.optimization_barrier(jnp.sum(jnp.cumsum(onehot, axis=1) * onehot, axis=-1)) - 1
    row_index = (jnp.arange(sources, dtype=jnp.int32)[:, None] * CAP + slot).reshape(-1).astype(jnp.int32)
    flat_ids = expert_ids.reshape(-1)
    token_rows = jnp.repeat(normed, TOPK, axis=0)
    buffer_rows = sources * CAP

    def one_expert(expert, total):
        chosen = flat_ids == expert
        index = jnp.where(chosen, row_index, buffer_rows).astype(jnp.int32)
        buffer = jnp.zeros((buffer_rows, D), jnp.bfloat16).at[index].set(token_rows, mode='drop')
        result = expert_rows(buffer, gate_weight[expert], up_weight[expert], down_weight[expert])
        picked = result[jnp.minimum(index, buffer_rows - 1)]
        picked = jnp.where(chosen[:, None], picked.astype(jnp.float32), 0.0).reshape(TOKENS, TOPK, D)
        return total + lax.optimization_barrier(jnp.sum(picked * route_weights[:, :, None], axis=1))
    total = lax.fori_loop(0, EXPERTS, one_expert, jnp.zeros((TOKENS, D), jnp.float32))
    return total.astype(jnp.bfloat16)
```

```python
import functools

import jax
import jax.numpy as jnp
from jax import lax
from jax.experimental import pallas as pl
from jax.experimental.pallas import tpu as pltpu
from jax.sharding import PartitionSpec as P

MESH = pl.DeviceIdType.MESH
LINE = 4
CHUNKS = 4


def kernel(
    planes, raw, gain, bias, ids, rw, gw, uw, dw, out,
    src, oth, tok, met, wg, wu, wd, sel, mix, snd, xin, hid, res, ret, psend, racc, obuf,
    s_own, s_wl, s_ws, s_wr, s_tok, s_toks, s_met, s_mets, s_os, s_x, s_xs, s_xd, s_xds,
    s_h, s_hs, s_r, s_rs, s_p, s_ps, s_ol, s_or, s_od,
):
    n = LINE
    side = planes
    me, core = lax.axis_index("ep"), lax.axis_index("tp")
    other = 1 - core
    z, p = me // side, lax.rem(me, side)
    tokens, width = raw.shape
    half = gw.shape[2]
    span = width // 2
    rows = snd.shape[2]
    cap = rows // side
    k = CHUNKS
    wide = span // k
    end = (z == 0) | (z == n - 1)
    mid = jnp.logical_not(end)
    step = jnp.where(z < n // 2, 1, -1)
    za, zb = z + step, z - step
    order = [
        z,
        jnp.where(end, z + 3 * step, z + 2 * step),
        jnp.where(end, z + 2 * step, z - step),
        z + step,
    ]

    def cols(c):
        return pl.ds(pl.multiple_of(c * wide, wide), wide)

    def part(h, size):
        return pl.ds(pl.multiple_of(h * size, size), size)

    def band(i):
        return pl.ds(pl.multiple_of(i * cap, cap), cap)

    def plane(t):
        return {"ep": t * side + p}

    partner = {"tp": other}

    def peer(j):
        return lax.rem(p + j, side)

    def remote(src, dst, send, recv, where):
        pltpu.make_async_remote_copy(
            src_ref=src, dst_ref=dst, send_sem=send, recv_sem=recv,
            device_id=where, device_id_type=MESH,
        ).start()

    def landed(ref, sem):
        pltpu.make_async_copy(ref, ref, sem).wait()

    barrier = pltpu.get_barrier_semaphore()
    own = pltpu.make_async_copy(raw, src, s_own)
    own.start()

    def greet(where):
        pl.semaphore_signal(barrier, inc=1, device_id=where, device_id_type=MESH)

    greet(partner)
    greet(plane(za))

    @pl.when(mid)
    def _():
        greet(plane(zb))

    for j in range(1, side):
        greet({"ep": z * side + peer(j)})

    mine = part(core, half)
    loads = [
        (gw.at[0], wg), (uw.at[0], wu), (dw.at[0, :, part(core, span)], wd.at[mine]),
    ]
    for i, (a, b) in enumerate(loads):
        pltpu.make_async_copy(a, b, s_wl.at[i]).start()

    met[z, core, 0:2, :] = ids[...].astype(jnp.float32)
    met[z, core, 2:4, :] = rw[...]

    own.wait()
    slab = min(32, tokens)

    @pl.loop(0, tokens // slab)
    def _(i):
        at = pl.ds(pl.multiple_of(i * slab, slab), slab)
        v = src[at, :].astype(jnp.float32)
        v = v - jnp.mean(v, axis=-1, keepdims=True)
        spread = jnp.mean(v * v, axis=-1, keepdims=True)
        y = v * lax.rsqrt(spread + 1e-05) * gain[...] + bias[...]
        y = y.astype(jnp.bfloat16)
        lo, hi = y[:, :span], y[:, span:]
        tok[z, core, at, :] = jnp.where(core == 0, lo, hi)
        oth[at, :] = jnp.where(core == 0, hi, lo)

    pl.semaphore_wait(barrier, side + 1 + jnp.where(mid, 1, 0))

    remote(met.at[z, core], met.at[z, core], s_os.at[0], s_met.at[z, core], partner)
    for c in range(k):
        remote(
            oth.at[:, cols(c)], tok.at[z, core, :, cols(c)], s_os.at[1], s_tok.at[z, core, c], partner
        )
    remote(
        dw.at[0, :, part(other, span)], wd.at[mine], s_ws, s_wr, partner
    )

    def send_tok(s, b, c, to, way):
        at = tok.at[s, b, :, cols(c)]
        remote(at, at, s_toks.at[way, s, b], s_tok.at[s, b, c], plane(to))

    def send_met(s, b, to, way):
        at = met.at[s, b]
        remote(at, at, s_mets.at[way, s, b], s_met.at[s, b], plane(to))

    def arrived(s, b, c):
        landed(tok.at[s, b, :, cols(c)], s_tok.at[s, b, c])

    def got_met(s, b):
        landed(met.at[s, b], s_met.at[s, b])

    def own_tok(b):
        for c in range(k):
            @pl.when(core != b)
            def _():
                arrived(z, b, c)

            send_tok(z, b, c, za, 0)

    def own_tok_b(b):
        for c in range(k):
            send_tok(z, b, c, zb, 1)

    def prep(q, b, s=None):
        s = order[q] if s is None else s
        ids0, ids1 = met[s, b, 0:1, :], met[s, b, 1:2, :]
        wt0, wt1 = met[s, b, 2:3, :], met[s, b, 3:4, :]
        row = lax.broadcasted_iota(jnp.int32, (rows, tokens), 0)
        e_row = (z * side + row // cap).astype(jnp.float32)
        s_row = lax.rem(row, cap).astype(jnp.float32)
        hit0 = (ids0 == e_row).astype(jnp.float32)
        hit1 = (ids1 == e_row).astype(jnp.float32)
        hit = hit0 + hit1
        before = (
            lax.broadcasted_iota(jnp.int32, (tokens, tokens), 0)
            < lax.broadcasted_iota(jnp.int32, (tokens, tokens), 1)
        ).astype(jnp.float32).astype(jnp.bfloat16)
        count = jnp.dot(hit.astype(jnp.bfloat16), before, preferred_element_type=jnp.float32)
        pick = jnp.where(count == s_row, hit, 0.0)
        sel[q, b] = pick.astype(jnp.bfloat16)
        w = (pick * (hit0 * wt0 + hit1 * wt1)).T
        high = w.astype(jnp.bfloat16)
        mix[q, b, 0] = high
        mix[q, b, 1] = (w - high.astype(jnp.float32)).astype(jnp.bfloat16)

    def disp(q, b, c, s=None):
        s = order[q] if s is None else s
        y = jnp.dot(sel[q, b], tok[s, b, :, cols(c)], preferred_element_type=jnp.float32)
        snd[q, b, :, cols(c)] = y.astype(jnp.bfloat16)
        xin[q, b, core, band(p), cols(c)] = snd[q, b, band(p), cols(c)]
        for j in range(1, side):
            o = peer(j)
            remote(
                snd.at[q, b, band(o), cols(c)], xin.at[q, b, core, band(p), cols(c)],
                s_xs.at[q, b], s_x.at[q, b], {"ep": z * side + o},
            )

    def others(ref):
        return ref.at[pl.ds(0, (side - 1) * cap)]

    def swap_x(q, b):
        landed(others(xin.at[q, b, core]), s_x.at[q, b])
        at = xin.at[q, b, core]
        remote(at, at, s_xds.at[q, b], s_xd.at[q, b], partner)

    tile = min(256, half)

    def gate(q, b):
        landed(xin.at[q, b, other], s_xd.at[q, b])

        @pl.loop(0, half // tile)
        def _(i):
            at = part(i, tile)
            lo, hi = xin[q, b, 0], xin[q, b, 1]
            g = jnp.dot(lo, wg[:span, at], preferred_element_type=jnp.float32)
            g = g + jnp.dot(hi, wg[span:, at], preferred_element_type=jnp.float32)
            u = jnp.dot(lo, wu[:span, at], preferred_element_type=jnp.float32)
            u = u + jnp.dot(hi, wu[span:, at], preferred_element_type=jnp.float32)
            v = g / (1.0 + jnp.exp(-g)) * u
            hid[q, b, core, :, at] = v.astype(jnp.bfloat16)

        at = hid.at[q, b, core]
        remote(at, at, s_hs.at[q, b], s_h.at[q, b], partner)

    def down(q, b, c):
        @pl.when(c == 0)
        def _():
            landed(hid.at[q, b, other], s_h.at[q, b])

        y = jnp.dot(hid[q, b, 0], wd[:half, cols(c)], preferred_element_type=jnp.float32)
        y = y + jnp.dot(hid[q, b, 1], wd[half:, cols(c)], preferred_element_type=jnp.float32)
        res[q, b, :, cols(c)] = y.astype(jnp.bfloat16)
        ret[q, b, band(p), cols(c)] = res[q, b, band(p), cols(c)]
        for j in range(1, side):
            o = peer(j)
            remote(
                res.at[q, b, band(o), cols(c)], ret.at[q, b, band(p), cols(c)],
                s_rs.at[q, b], s_r.at[q, b, c], {"ep": z * side + o},
            )

    def downs(q, b):
        pl.loop(0, k)(lambda c: down(q, b, c))

    def weigh(q, b, c):
        landed(others(ret.at[q, b, :, cols(c)]), s_r.at[q, b, c])
        r = ret[q, b, :, cols(c)]
        return jnp.dot(mix[q, b, 0], r, preferred_element_type=jnp.float32) + jnp.dot(
            mix[q, b, 1], r, preferred_element_type=jnp.float32
        )

    def combine(q, b, c, t, to, add):
        y = weigh(q, b, c)
        if add:
            landed(racc.at[t, b, c], s_p.at[t, b, c])
            y = y + racc[t, b, c].astype(jnp.float32)
        psend[q - 1, b, c] = y.astype(jnp.bfloat16)
        slot = jnp.where((to == t) & (to < z), n, t)
        remote(
            psend.at[q - 1, b, c], racc.at[slot, b, c], s_ps.at[q - 1, b], s_p.at[slot, b, c], plane(to)
        )

    def weights():
        for i, (a, b) in enumerate(loads):
            pltpu.make_async_copy(a, b, s_wl.at[i]).wait()
        landed(wd.at[part(other, half)], s_wr)

    def own_met(b):
        send_met(z, b, za, 0)

        @pl.when(mid)
        def _():
            send_met(z, b, zb, 1)

    own_met(core)
    own_tok(0)

    @pl.when(mid)
    def _():
        own_tok_b(0)

    got_met(z, other)
    own_met(other)
    prep(0, 0)
    pl.loop(0, k)(lambda c: disp(0, 0, c))

    @pl.when(end)
    def _():
        own_tok(1)

    @pl.when(mid)
    def _():
        @pl.when(core != 1)
        def _():
            for c in range(k):
                arrived(z, 1, c)

    prep(0, 1)

    @pl.when(mid)
    def _():
        def relay(q, b, c):
            s = order[q]
            arrived(s, b, c)
            send_tok(s, b, c, za if q == 2 else zb, 0 if q == 2 else 1)

        def learn(q, b):
            got_met(order[q], b)
            send_met(order[q], b, za if q == 2 else zb, 0 if q == 2 else 1)
            prep(q, b)

        def fold(q, b, c):
            combine(q, b, c, order[q], zb if q == 2 else za, True)

        def folds(q, b, lo, hi):
            pl.loop(lo, hi)(lambda c: fold(q, b, c))

        learn(3, 0)
        learn(2, 0)

        @pl.loop(0, k)
        def _(c):
            relay(3, 0, c)
            relay(2, 0, c)
            disp(3, 0, c)
            disp(0, 1, c)

        learn(1, 0)
        learn(2, 1)

        @pl.loop(0, k)
        def _(c):
            relay(1, 0, c)
            relay(2, 1, c)
            disp(1, 0, c)
            disp(2, 0, c)

            @pl.when(c == 0)
            def _():
                weights()
                swap_x(0, 0)

            @pl.when(c == 1)
            def _():
                swap_x(3, 0)
                gate(0, 0)

            @pl.when(c == 2)
            def _():
                gate(3, 0)

        pl.loop(0, k)(lambda c: send_tok(z, 1, c, za, 0))
        learn(1, 1)

        @pl.loop(0, k)
        def _(c):
            relay(1, 1, c)
            disp(1, 1, c)
            down(3, 0, c)

            @pl.when(c == 1)
            def _():
                swap_x(0, 1)
                swap_x(1, 0)

            @pl.when(c == 2)
            def _():
                gate(1, 0)

        learn(3, 1)
        gate(0, 1)

        @pl.loop(0, k)
        def _(c):
            relay(3, 1, c)
            disp(3, 1, c)
            down(1, 0, c)

            @pl.when(c == 0)
            def _():
                swap_x(2, 0)

            @pl.when(c == 1)
            def _():
                swap_x(1, 1)
                gate(2, 0)

            @pl.when(c == 2)
            def _():
                gate(1, 1)

            @pl.when(c > 0)
            def _():
                fold(3, 0, c - 1)

        pl.loop(0, k)(lambda c: send_tok(z, 1, c, zb, 1))
        pl.loop(0, k)(lambda c: disp(2, 1, c))
        fold(3, 0, k - 1)
        downs(1, 1)
        folds(1, 0, 0, k // 2)
        swap_x(3, 1)
        downs(2, 0)
        folds(1, 0, k // 2, k)
        swap_x(2, 1)
        gate(3, 1)
        downs(3, 1)
        gate(2, 1)

        @pl.loop(0, k // 2)
        def _(c):
            fold(1, 1, c)
            fold(2, 0, c)

        downs(2, 1)

        @pl.loop(k // 2, k)
        def _(c):
            fold(1, 1, c)
            fold(2, 0, c)

        downs(0, 0)

        @pl.loop(0, k // 2)
        def _(c):
            fold(3, 1, c)
            fold(2, 1, c)

        downs(0, 1)

        @pl.loop(k // 2, k)
        def _(c):
            fold(3, 1, c)
            fold(2, 1, c)

    @pl.when(end)
    def _():
        pl.loop(0, k)(lambda c: disp(0, 1, c))

        def take(q, b, c):
            s = z + (n - q) * step
            arrived(s, b, c)
            disp(q, b, c, s)

        def learn(q, b):
            s = z + (n - q) * step
            got_met(s, b)
            prep(q, b, s)

        def unit(i):
            return jnp.where(i < 3, 3 - i, i - 2), jnp.where(i < 3, 0, 1)

        def fold(q, b, c):
            combine(q, b, c, z + (n - q) * step, za, False)

        learn(3, 0)

        @pl.loop(0, k)
        def _(c):
            take(3, 0, c)

            @pl.when(c == 1)
            def _():
                weights()
                swap_x(0, 0)

            @pl.when(c == 2)
            def _():
                gate(0, 0)

        quarter = k // 4

        @pl.loop(0, 5)
        def _(i):
            q, b = unit(i)
            q1, b1 = unit(i + 1)
            q0, b0 = unit(jnp.maximum(i - 1, 0))

            def more(j):
                pl.loop(j * quarter, (j + 1) * quarter)(lambda c: take(q1, b1, c))

            def back(j):
                pl.when(i > 0)(lambda: pl.loop(j * quarter, (j + 1) * quarter)(lambda c: fold(q0, b0, c)))

            learn(q1, b1)
            more(0)
            swap_x(q, b)
            back(1)
            more(1)
            gate(q, b)
            back(2)
            more(2)
            pl.loop(0, k // 2)(lambda c: down(q, b, c))
            back(3)
            more(3)
            pl.loop(k // 2, k)(lambda c: down(q, b, c))
            pl.loop(0, quarter)(lambda c: fold(q, b, c))

            @pl.when(i == 0)
            def _():
                swap_x(0, 1)
                downs(0, 0)
                gate(0, 1)

        swap_x(3, 1)
        pl.loop(quarter, 2 * quarter)(lambda c: fold(2, 1, c))
        gate(3, 1)
        pl.loop(2 * quarter, k)(lambda c: fold(2, 1, c))
        downs(3, 1)
        downs(0, 1)
        pl.loop(0, k)(lambda c: fold(3, 1, c))

    def last(b, c, slots):
        y = weigh(0, b, c)
        for slot in slots:
            landed(racc.at[slot, b, c], s_p.at[slot, b, c])
            y = y + racc[slot, b, c].astype(jnp.float32)
        obuf[b, c] = y.astype(out.dtype)
        to = out.at[:, pl.ds(pl.multiple_of(core * span + c * wide, wide), wide)]

        @pl.when(core == b)
        def _():
            pltpu.make_async_copy(obuf.at[b, c], to, s_ol).start()

        @pl.when(core != b)
        def _():
            remote(obuf.at[b, c], to, s_od, s_or, partner)

    @pl.when(end)
    def _():
        for b in range(2):
            pl.loop(0, k)(lambda c: last(b, c, [jnp.where(z == 0, n, z)]))

    @pl.when(mid)
    def _():
        for b in range(2):
            pl.loop(0, k)(lambda c: last(b, c, [z, n]))

    drain = landed
    drain(met.at[z, core], s_os.at[0])
    drain(oth, s_os.at[1])
    drain(wd.at[mine], s_ws)
    for b in range(2):
        drain(tok.at[z, b], s_toks.at[0, z, b])
        drain(met.at[z, b], s_mets.at[0, z, b])

    @pl.when(mid)
    def _():
        for b in range(2):
            for way, s in ((1, z), (0, order[2]), (1, order[1]), (1, order[3])):
                drain(tok.at[s, b], s_toks.at[way, s, b])
                drain(met.at[s, b], s_mets.at[way, s, b])

    for q in range(n):
        for b in range(2):
            drain(others(snd.at[q, b]), s_xs.at[q, b])
            drain(others(res.at[q, b]), s_rs.at[q, b])
            drain(xin.at[q, b, core], s_xds.at[q, b])
            drain(hid.at[q, b, core], s_hs.at[q, b])
            if q > 0:
                drain(psend.at[q - 1, b], s_ps.at[q - 1, b])
    drain(obuf.at[0], s_ol)
    drain(obuf.at[0], s_od)
    drain(obuf.at[0], s_or)


def body(
    tokens, norm_gain, norm_bias, gate_weight, up_weight, down_weight, expert_ids, route_weights
):
    count, width = tokens.shape
    experts = lax.axis_size("ep")
    cap = max(4 * count // experts, 4)
    side = experts // LINE
    half = gate_weight.shape[2]
    rows = side * cap
    span = width // 2
    wide = span // CHUNKS
    bf = jnp.bfloat16
    dma = pltpu.SemaphoreType.DMA
    vmem = pl.BlockSpec(memory_space=pltpu.VMEM)
    hbm = pl.BlockSpec(memory_space=pl.ANY)
    return pl.pallas_call(
        functools.partial(kernel, side),
        out_shape=jax.ShapeDtypeStruct((count, width), bf),
        in_specs=[hbm] + [vmem] * 4 + [hbm] * 3,
        out_specs=hbm,
        scratch_shapes=[
            pltpu.VMEM((count, width), bf),
            pltpu.VMEM((count, span), bf),
            pltpu.VMEM((LINE, 2, count, span), bf),
            pltpu.VMEM((LINE, 2, 8, count), jnp.float32),
            pltpu.VMEM((width, half), bf),
            pltpu.VMEM((width, half), bf),
            pltpu.VMEM((2 * half, span), bf),
            pltpu.VMEM((LINE, 2, rows, count), bf),
            pltpu.VMEM((LINE, 2, 2, count, rows), bf),
            pltpu.VMEM((LINE, 2, rows, span), bf),
            pltpu.VMEM((LINE, 2, 2, rows, span), bf),
            pltpu.VMEM((LINE, 2, 2, rows, half), bf),
            pltpu.VMEM((LINE, 2, rows, span), bf),
            pltpu.VMEM((LINE, 2, rows, span), bf),
            pltpu.VMEM((LINE - 1, 2, CHUNKS, count, wide), bf),
            pltpu.VMEM((LINE + 1, 2, CHUNKS, count, wide), bf),
            pltpu.VMEM((2, CHUNKS, count, wide), bf),
            dma,
            dma((3,)),
            dma,
            dma,
            dma((LINE, 2, CHUNKS)),
            dma((2, LINE, 2)),
            dma((LINE, 2)),
            dma((2, LINE, 2)),
            dma((2,)),
            dma((LINE, 2)),
            dma((LINE, 2)),
            dma((LINE, 2)),
            dma((LINE, 2)),
            dma((LINE, 2)),
            dma((LINE, 2)),
            dma((LINE, 2, CHUNKS)),
            dma((LINE, 2)),
            dma((LINE + 1, 2, CHUNKS)),
            dma((LINE - 1, 2)),
            dma,
            dma,
            dma,
        ],
        compiler_params=pltpu.CompilerParams(
            collective_id=0, has_side_effects=True, vmem_limit_bytes=60 * 1024 * 1024
        ),
    )(
        tokens, norm_gain[None], norm_bias[None], expert_ids.T, route_weights.T,
        gate_weight, up_weight, down_weight,
    )


def solution(mesh):
    placed = (
        P(("ep", "tp"), None),
        P(),
        P(),
        P("ep", None, "tp"),
        P("ep", None, "tp"),
        P("ep", "tp", None),
        P(("ep", "tp"), None),
        P(("ep", "tp"), None),
    )
    return jax.shard_map(
        body, mesh=mesh, in_specs=placed, out_specs=P(("ep", "tp"), None), check_vma=False
    )
```

```python
import functools

import jax
import jax.numpy as jnp
from jax import lax
from jax.experimental import pallas as pl
from jax.experimental.pallas import tpu as pltpu
from jax.sharding import PartitionSpec as P

MESH = pl.DeviceIdType.MESH
LINE = 4
CHUNKS = 4


def kernel(
    planes, raw, gain_in, bias_in, ids_in, rw_in, gw, uw, dw, out,
    src, gain, bias, ids, rw, oth, tok, met, wg, wu, wd, sel, mix, snd, xin, hid, res, ret, psend, racc, obuf,
    s_own, s_lent, s_wl, s_ws, s_wr, s_tok, s_toks, s_met, s_mets, s_os, s_x, s_xs, s_xd, s_xds,
    s_h, s_hs, s_r, s_rs, s_p, s_ps, s_or, s_od,
):
    n = LINE
    side = planes
    me, core = lax.axis_index("ep"), lax.axis_index("tp")
    other = 1 - core
    z, p = me // side, lax.rem(me, side)
    tokens, width = raw.shape
    half = gw.shape[2]
    span = width // 2
    rows = snd.shape[2]
    cap = rows // side
    k = CHUNKS
    wide = span // k
    end = (z == 0) | (z == n - 1)
    mid = jnp.logical_not(end)
    step = jnp.where(z < n // 2, 1, -1)
    za, zb = z + step, z - step
    order = [
        z,
        jnp.where(end, z + 3 * step, z + 2 * step),
        jnp.where(end, z + 2 * step, z - step),
        z + step,
    ]

    def cols(c):
        return pl.ds(pl.multiple_of(c * wide, wide), wide)

    def part(h, size):
        return pl.ds(pl.multiple_of(h * size, size), size)

    def band(i):
        return pl.ds(pl.multiple_of(i * cap, cap), cap)

    def plane(t):
        return {"ep": t * side + p}

    partner = {"tp": other}

    def peer(j):
        return lax.rem(p + j, side)

    def remote(src, dst, send, recv, where):
        pltpu.make_async_remote_copy(
            src_ref=src, dst_ref=dst, send_sem=send, recv_sem=recv,
            device_id=where, device_id_type=MESH,
        ).start()

    def landed(ref, sem):
        pltpu.make_async_copy(ref, ref, sem).wait()

    barrier = pltpu.get_barrier_semaphore()
    small = [(ids_in, ids), (rw_in, rw), (gain_in, gain), (bias_in, bias)]
    slab = min(64, tokens)
    turns = tokens // slab

    def fetch(i):
        at = part(i, slab)
        return pltpu.make_async_copy(raw.at[at], src.at[at], s_own.at[len(small) + i])

    fetch(0).start()
    for i, (a, b) in enumerate(small):
        pltpu.make_async_copy(a, b, s_own.at[i]).start()
    for i in range(1, turns):
        fetch(i).start()

    def greet(where):
        pl.semaphore_signal(barrier, inc=1, device_id=where, device_id_type=MESH)

    greet(partner)
    greet(plane(za))

    @pl.when(mid)
    def _():
        greet(plane(zb))

    for j in range(1, side):
        greet({"ep": z * side + peer(j)})

    mine = part(core, half)
    loads = [
        (gw.at[0], wg), (uw.at[0], wu), (dw.at[0, :, part(core, span)], wd.at[mine]),
    ]
    for i, (a, b) in enumerate(loads):
        pltpu.make_async_copy(a, b, s_wl.at[i]).start()

    for i, (a, b) in enumerate(small):
        pltpu.make_async_copy(a, b, s_own.at[i]).wait()
    met[z, core, 0:2, :] = ids[...].astype(jnp.float32)
    met[z, core, 2:4, :] = rw[...]

    def lnorm(i):
        fetch(i).wait()
        at = part(i, slab)
        v = src[at, :].astype(jnp.float32)
        v = v - jnp.mean(v, axis=-1, keepdims=True)
        spread = jnp.mean(v * v, axis=-1, keepdims=True)
        y = v * lax.rsqrt(spread + 1e-05) * gain[...] + bias[...]
        y = y.astype(jnp.bfloat16)
        lo, hi = y[:, :span], y[:, span:]
        tok[z, core, at, :] = jnp.where(core == 0, lo, hi)
        oth[at, :] = jnp.where(core == 0, hi, lo)

    def waitbar():
        pl.semaphore_wait(barrier, side + 1 + jnp.where(mid, 1, 0))

    block = tokens // 2

    def lend(h):
        at = part(h, block)
        remote(oth.at[at], tok.at[z, core, at], s_os.at[1], s_lent.at[h], partner)

    pl.loop(0, turns // 2)(lnorm)
    waitbar()
    remote(met.at[z, core], met.at[z, core], s_os.at[0], s_met.at[z, core], partner)
    lend(0)
    pl.loop(turns // 2, turns)(lnorm)
    lend(1)

    remote(
        dw.at[0, :, part(other, span)], wd.at[mine], s_ws, s_wr, partner
    )

    def send_tok(s, b, c, to, way):
        at = tok.at[s, b, :, cols(c)]
        remote(at, at, s_toks.at[way, s, b], s_tok.at[s, b, c], plane(to))

    def send_met(s, b, to, way):
        at = met.at[s, b]
        remote(at, at, s_mets.at[way, s, b], s_met.at[s, b], plane(to))

    def arrived(s, b, c):
        landed(tok.at[s, b, :, cols(c)], s_tok.at[s, b, c])

    def got_met(s, b):
        landed(met.at[s, b], s_met.at[s, b])

    def lent():
        for h in range(2):
            landed(oth.at[part(h, block)], s_lent.at[h])

    def own_tok(b, lo, hi):
        for c in range(lo, hi):
            send_tok(z, b, c, za, 0)

            if b == 0:
                @pl.when(mid)
                def _():
                    send_tok(z, b, c, zb, 1)

    def prep(q, b, s=None):
        s = order[q] if s is None else s
        ids0, ids1 = met[s, b, 0:1, :], met[s, b, 1:2, :]
        wt0, wt1 = met[s, b, 2:3, :], met[s, b, 3:4, :]
        row = lax.broadcasted_iota(jnp.int32, (rows, tokens), 0)
        e_row = (z * side + row // cap).astype(jnp.float32)
        s_row = lax.rem(row, cap).astype(jnp.float32)
        hit0 = (ids0 == e_row).astype(jnp.float32)
        hit1 = (ids1 == e_row).astype(jnp.float32)
        hit = hit0 + hit1
        before = (
            lax.broadcasted_iota(jnp.int32, (tokens, tokens), 0)
            < lax.broadcasted_iota(jnp.int32, (tokens, tokens), 1)
        ).astype(jnp.float32).astype(jnp.bfloat16)
        count = jnp.dot(hit.astype(jnp.bfloat16), before, preferred_element_type=jnp.float32)
        pick = jnp.where(count == s_row, hit, 0.0)
        sel[q, b] = pick.astype(jnp.bfloat16)
        w = (pick * (hit0 * wt0 + hit1 * wt1)).T
        high = w.astype(jnp.bfloat16)
        mix[q, b, 0] = high
        mix[q, b, 1] = (w - high.astype(jnp.float32)).astype(jnp.bfloat16)

    def disp(q, b, c, s=None):
        s = order[q] if s is None else s
        y = jnp.dot(sel[q, b], tok[s, b, :, cols(c)], preferred_element_type=jnp.float32)
        snd[q, b, :, cols(c)] = y.astype(jnp.bfloat16)
        xin[q, b, core, band(p), cols(c)] = snd[q, b, band(p), cols(c)]
        for j in range(1, side):
            o = peer(j)
            remote(
                snd.at[q, b, band(o), cols(c)], xin.at[q, b, core, band(p), cols(c)],
                s_xs.at[q, b], s_x.at[q, b, c], {"ep": z * side + o},
            )

    def others(ref):
        return ref.at[pl.ds(0, (side - 1) * cap)]

    def swap_x(q, b):
        @pl.loop(0, k)
        def _(c):
            at = xin.at[q, b, core, :, cols(c)]
            landed(others(at), s_x.at[q, b, c])
            remote(at, at, s_xds.at[q, b], s_xd.at[q, b], partner)

    tile = min(256, half)

    def gate(q, b):
        landed(xin.at[q, b, other], s_xd.at[q, b])

        @pl.loop(0, half // tile)
        def _(i):
            at = part(i, tile)
            lo, hi = xin[q, b, 0], xin[q, b, 1]
            g = jnp.dot(lo, wg[:span, at], preferred_element_type=jnp.float32)
            g = g + jnp.dot(hi, wg[span:, at], preferred_element_type=jnp.float32)
            u = jnp.dot(lo, wu[:span, at], preferred_element_type=jnp.float32)
            u = u + jnp.dot(hi, wu[span:, at], preferred_element_type=jnp.float32)
            v = g / (1.0 + jnp.exp(-g)) * u
            hid[q, b, core, :, at] = v.astype(jnp.bfloat16)
            done = hid.at[q, b, core, :, at]
            remote(done, done, s_hs.at[q, b], s_h.at[q, b], partner)

    def down(q, b, c):
        @pl.when(c == 0)
        def _():
            landed(hid.at[q, b, other], s_h.at[q, b])

        y = jnp.dot(hid[q, b, 0], wd[:half, cols(c)], preferred_element_type=jnp.float32)
        y = y + jnp.dot(hid[q, b, 1], wd[half:, cols(c)], preferred_element_type=jnp.float32)
        res[q, b, :, cols(c)] = y.astype(jnp.bfloat16)
        ret[q, b, band(p), cols(c)] = res[q, b, band(p), cols(c)]
        for j in range(1, side):
            o = peer(j)
            remote(
                res.at[q, b, band(o), cols(c)], ret.at[q, b, band(p), cols(c)],
                s_rs.at[q, b], s_r.at[q, b, c], {"ep": z * side + o},
            )

    def downs(q, b):
        pl.loop(0, k)(lambda c: down(q, b, c))

    def weigh(q, b, c):
        landed(others(ret.at[q, b, :, cols(c)]), s_r.at[q, b, c])
        r = ret[q, b, :, cols(c)]
        return jnp.dot(mix[q, b, 0], r, preferred_element_type=jnp.float32) + jnp.dot(
            mix[q, b, 1], r, preferred_element_type=jnp.float32
        )

    def combine(q, b, c, t, to, add):
        y = weigh(q, b, c)
        if add:
            landed(racc.at[t, b, c], s_p.at[t, b, c])
            y = y + racc[t, b, c].astype(jnp.float32)
        psend[q - 1, b, c] = y.astype(jnp.bfloat16)
        slot = jnp.where((to == t) & (to < z), n, t)
        remote(
            psend.at[q - 1, b, c], racc.at[slot, b, c], s_ps.at[q - 1, b], s_p.at[slot, b, c], plane(to)
        )

    def weights():
        for i, (a, b) in enumerate(loads):
            pltpu.make_async_copy(a, b, s_wl.at[i]).wait()
        landed(wd.at[part(other, half)], s_wr)

    def own_met(b):
        send_met(z, b, za, 0)

        @pl.when(mid)
        def _():
            send_met(z, b, zb, 1)

    own_met(core)
    pl.when(core == 1)(lent)
    own_tok(0, 0, 1)
    got_met(z, other)
    own_met(other)
    own_tok(0, 1, k)
    prep(0, 0)
    pl.loop(0, k)(lambda c: disp(0, 0, c))

    pl.when(core == 0)(lent)

    @pl.when(end)
    def _():
        own_tok(1, 0, k)

    prep(0, 1)

    @pl.when(mid)
    def _():
        def relay(q, b, c):
            s = order[q]
            arrived(s, b, c)
            send_tok(s, b, c, za if q == 2 else zb, 0 if q == 2 else 1)

        def learn(q, b):
            got_met(order[q], b)
            send_met(order[q], b, za if q == 2 else zb, 0 if q == 2 else 1)
            prep(q, b)

        def fold(q, b, c):
            combine(q, b, c, order[q], zb if q == 2 else za, True)

        def folds(q, b, lo, hi):
            pl.loop(lo, hi)(lambda c: fold(q, b, c))

        learn(3, 0)
        learn(2, 0)

        @pl.loop(0, k)
        def _(c):
            relay(3, 0, c)
            relay(2, 0, c)
            disp(3, 0, c)
            disp(0, 1, c)

        learn(1, 0)
        learn(2, 1)

        @pl.loop(0, k)
        def _(c):
            relay(1, 0, c)
            relay(2, 1, c)
            disp(1, 0, c)
            disp(2, 0, c)

            @pl.when(c == 0)
            def _():
                weights()
                swap_x(0, 0)

            @pl.when(c == 1)
            def _():
                swap_x(3, 0)
                gate(0, 0)

            @pl.when(c == 2)
            def _():
                gate(3, 0)

        pl.loop(0, k)(lambda c: send_tok(z, 1, c, za, 0))
        learn(1, 1)

        @pl.loop(0, k)
        def _(c):
            relay(1, 1, c)
            disp(1, 1, c)
            down(3, 0, c)

            @pl.when(c == 1)
            def _():
                swap_x(0, 1)
                swap_x(1, 0)

            @pl.when(c == 2)
            def _():
                gate(1, 0)

        learn(3, 1)
        gate(0, 1)

        @pl.loop(0, k)
        def _(c):
            relay(3, 1, c)
            disp(3, 1, c)
            down(1, 0, c)

            @pl.when(c == 0)
            def _():
                swap_x(2, 0)

            @pl.when(c == 1)
            def _():
                swap_x(1, 1)
                gate(2, 0)

            @pl.when(c == 2)
            def _():
                gate(1, 1)

        pl.loop(0, k)(lambda c: send_tok(z, 1, c, zb, 1))
        pl.loop(0, k)(lambda c: disp(2, 1, c))
        folds(3, 0, 0, k)
        downs(1, 1)
        folds(1, 0, 0, k // 2)
        swap_x(3, 1)
        downs(2, 0)
        folds(1, 0, k // 2, k)
        swap_x(2, 1)
        gate(3, 1)
        downs(3, 1)
        gate(2, 1)

        @pl.loop(0, k // 2)
        def _(c):
            fold(1, 1, c)
            fold(2, 0, c)

        downs(2, 1)

        @pl.loop(k // 2, k)
        def _(c):
            fold(1, 1, c)
            fold(2, 0, c)

        downs(0, 0)

        @pl.loop(0, k // 2)
        def _(c):
            fold(3, 1, c)
            fold(2, 1, c)

        downs(0, 1)

        @pl.loop(k // 2, k)
        def _(c):
            fold(3, 1, c)
            fold(2, 1, c)

    @pl.when(end)
    def _():
        def take(q, b, c):
            s = z + (n - q) * step
            arrived(s, b, c)
            disp(q, b, c, s)

        def learn(q, b):
            s = z + (n - q) * step
            got_met(s, b)
            prep(q, b, s)

        def unit(i):
            return jnp.where(i < 3, 3 - i, i - 2), jnp.where(i < 3, 0, 1)

        def fold(q, b, c):
            combine(q, b, c, z + (n - q) * step, za, False)

        learn(3, 0)

        @pl.loop(0, k)
        def _(c):
            take(3, 0, c)
            disp(0, 1, c)

            @pl.when(c == 1)
            def _():
                weights()
                swap_x(0, 0)

            @pl.when(c == 2)
            def _():
                gate(0, 0)

        pl.loop(0, k // 2)(lambda c: down(0, 0, c))
        quarter = k // 4

        @pl.loop(0, 5)
        def _(i):
            q, b = unit(i)
            q1, b1 = unit(i + 1)
            q0, b0 = unit(jnp.maximum(i - 1, 0))

            def more(j):
                pl.loop(j * quarter, (j + 1) * quarter)(lambda c: take(q1, b1, c))

            def back(j):
                pl.when(i > 0)(lambda: pl.loop(j * quarter, (j + 1) * quarter)(lambda c: fold(q0, b0, c)))

            learn(q1, b1)
            more(0)
            swap_x(q, b)
            back(1)
            more(1)
            gate(q, b)
            back(2)
            more(2)
            pl.loop(0, k // 2)(lambda c: down(q, b, c))
            back(3)
            more(3)
            pl.loop(k // 2, k)(lambda c: down(q, b, c))

            @pl.when(i == 1)
            def _():
                swap_x(0, 1)

            @pl.when(i == 2)
            def _():
                gate(0, 1)

            @pl.when(i == 4)
            def _():
                downs(0, 1)

            pl.loop(0, quarter)(lambda c: fold(q, b, c))

        swap_x(3, 1)
        pl.loop(quarter, 2 * quarter)(lambda c: fold(2, 1, c))
        gate(3, 1)
        pl.loop(2 * quarter, k)(lambda c: fold(2, 1, c))
        downs(3, 1)
        pl.loop(k // 2, k)(lambda c: down(0, 0, c))
        pl.loop(0, k)(lambda c: fold(3, 1, c))

    def last(b, c, slots):
        y = weigh(0, b, c)
        for slot in slots:
            landed(racc.at[slot, b, c], s_p.at[slot, b, c])
            y = y + racc[slot, b, c].astype(jnp.float32)
        to = pl.ds(pl.multiple_of(core * span + c * wide, wide), wide)

        @pl.when(core == b)
        def _():
            out[:, to] = y.astype(out.dtype)

        @pl.when(core != b)
        def _():
            obuf[c] = y.astype(out.dtype)
            remote(obuf.at[c], out.at[:, to], s_od, s_or, partner)

    @pl.when(end)
    def _():
        for b in range(2):
            pl.loop(0, k)(lambda c: last(b, c, [jnp.where(z == 0, n, z)]))

    @pl.when(mid)
    def _():
        for b in range(2):
            pl.loop(0, k)(lambda c: last(b, c, [z, n]))

    drain = landed
    drain(met.at[z, core], s_os.at[0])
    drain(oth, s_os.at[1])
    drain(wd.at[mine], s_ws)
    for b in range(2):
        drain(tok.at[z, b], s_toks.at[0, z, b])
        drain(met.at[z, b], s_mets.at[0, z, b])

    @pl.when(mid)
    def _():
        for b in range(2):
            for way, s in ((1, z), (0, order[2]), (1, order[1]), (1, order[3])):
                drain(tok.at[s, b], s_toks.at[way, s, b])
                drain(met.at[s, b], s_mets.at[way, s, b])

    for q in range(n):
        for b in range(2):
            drain(others(snd.at[q, b]), s_xs.at[q, b])
            drain(others(res.at[q, b]), s_rs.at[q, b])
            drain(xin.at[q, b, core], s_xds.at[q, b])
            drain(hid.at[q, b, core], s_hs.at[q, b])
            if q > 0:
                drain(psend.at[q - 1, b], s_ps.at[q - 1, b])
    drain(obuf, s_od)
    drain(obuf, s_or)


def body(
    tokens, norm_gain, norm_bias, gate_weight, up_weight, down_weight, expert_ids, route_weights
):
    count, width = tokens.shape
    experts = lax.axis_size("ep")
    cap = max(4 * count // experts, 4)
    side = experts // LINE
    half = gate_weight.shape[2]
    rows = side * cap
    span = width // 2
    wide = span // CHUNKS
    bf = jnp.bfloat16
    dma = pltpu.SemaphoreType.DMA
    hbm = pl.BlockSpec(memory_space=pl.ANY)
    return pl.pallas_call(
        functools.partial(kernel, side),
        out_shape=pltpu.VMEM((count, width), bf),
        in_specs=[hbm] * 8,
        out_specs=pl.BlockSpec(memory_space=pltpu.VMEM),
        scratch_shapes=[
            pltpu.VMEM((count, width), bf),
            pltpu.VMEM((1, width), jnp.float32),
            pltpu.VMEM((1, width), jnp.float32),
            pltpu.VMEM((2, count), jnp.int32),
            pltpu.VMEM((2, count), jnp.float32),
            pltpu.VMEM((count, span), bf),
            pltpu.VMEM((LINE, 2, count, span), bf),
            pltpu.VMEM((LINE, 2, 8, count), jnp.float32),
            pltpu.VMEM((width, half), bf),
            pltpu.VMEM((width, half), bf),
            pltpu.VMEM((2 * half, span), bf),
            pltpu.VMEM((LINE, 2, rows, count), bf),
            pltpu.VMEM((LINE, 2, 2, count, rows), bf),
            pltpu.VMEM((LINE, 2, rows, span), bf),
            pltpu.VMEM((LINE, 2, 2, rows, span), bf),
            pltpu.VMEM((LINE, 2, 2, rows, half), bf),
            pltpu.VMEM((LINE, 2, rows, span), bf),
            pltpu.VMEM((LINE, 2, rows, span), bf),
            pltpu.VMEM((LINE - 1, 2, CHUNKS, count, wide), bf),
            pltpu.VMEM((LINE + 1, 2, CHUNKS, count, wide), bf),
            pltpu.VMEM((CHUNKS, count, wide), bf),
            dma((4 + count // min(64, count),)),
            dma((2,)),
            dma((3,)),
            dma,
            dma,
            dma((LINE, 2, CHUNKS)),
            dma((2, LINE, 2)),
            dma((LINE, 2)),
            dma((2, LINE, 2)),
            dma((2,)),
            dma((LINE, 2, CHUNKS)),
            dma((LINE, 2)),
            dma((LINE, 2)),
            dma((LINE, 2)),
            dma((LINE, 2)),
            dma((LINE, 2)),
            dma((LINE, 2, CHUNKS)),
            dma((LINE, 2)),
            dma((LINE + 1, 2, CHUNKS)),
            dma((LINE - 1, 2)),
            dma,
            dma,
        ],
        compiler_params=pltpu.CompilerParams(
            collective_id=0, has_side_effects=True, vmem_limit_bytes=56 * 1024 * 1024
        ),
    )(
        tokens, norm_gain[None], norm_bias[None], expert_ids.T, route_weights.T,
        gate_weight, up_weight, down_weight,
    )


def solution(mesh):
    placed = (
        P(("ep", "tp"), None),
        P(),
        P(),
        P("ep", None, "tp"),
        P("ep", None, "tp"),
        P("ep", "tp", None),
        P(("ep", "tp"), None),
        P(("ep", "tp"), None),
    )
    return jax.shard_map(
        body, mesh=mesh, in_specs=placed, out_specs=P(("ep", "tp"), None), check_vma=False
    )
```

```python
import functools

import jax
import jax.numpy as jnp
from jax import lax
from jax.experimental import pallas as pl
from jax.experimental.pallas import tpu as pltpu
from jax.sharding import PartitionSpec as P

MESH = pl.DeviceIdType.MESH
LINE = 4
CHUNKS = 4


def kernel(
    planes, raw, gain_in, bias_in, ids_in, rw_in, gw, uw, dw, out,
    src, gain, bias, ids, rw, oth, tok, met, wg, wu, wd, sel, mix, snd, xin, hid, res, ret, psend, racc, obuf,
    s_own, s_lent, s_wl, s_ws, s_wr, s_tok, s_toks, s_met, s_mets, s_os, s_x, s_xs, s_xd, s_xds,
    s_h, s_hs, s_r, s_rs, s_p, s_ps, s_or, s_od,
):
    n = LINE
    side = planes
    me, core = lax.axis_index("ep"), lax.axis_index("tp")
    other = 1 - core
    z, p = me // side, lax.rem(me, side)
    tokens, width = raw.shape
    half = gw.shape[2]
    span = width // 2
    rows = snd.shape[2]
    cap = rows // side
    k = CHUNKS
    wide = span // k
    end = (z == 0) | (z == n - 1)
    mid = jnp.logical_not(end)
    step = jnp.where(z < n // 2, 1, -1)
    za, zb = z + step, z - step
    order = [
        z,
        jnp.where(end, z + 3 * step, z + 2 * step),
        jnp.where(end, z + 2 * step, z - step),
        z + step,
    ]

    def cols(c):
        return pl.ds(pl.multiple_of(c * wide, wide), wide)

    def part(h, size):
        return pl.ds(pl.multiple_of(h * size, size), size)

    def band(i):
        return pl.ds(pl.multiple_of(i * cap, cap), cap)

    def plane(t):
        return {"ep": t * side + p}

    partner = {"tp": other}

    def peer(j):
        return lax.rem(p + j, side)

    def remote(src, dst, send, recv, where):
        pltpu.make_async_remote_copy(
            src_ref=src, dst_ref=dst, send_sem=send, recv_sem=recv,
            device_id=where, device_id_type=MESH,
        ).start()

    def landed(ref, sem):
        pltpu.make_async_copy(ref, ref, sem).wait()

    barrier = pltpu.get_barrier_semaphore()
    small = [(ids_in, ids), (rw_in, rw), (gain_in, gain), (bias_in, bias)]
    slab = min(64, tokens)
    turns = tokens // slab

    def fetch(i):
        at = part(i, slab)
        return pltpu.make_async_copy(raw.at[at], src.at[at], s_own.at[len(small) + i])

    fetch(0).start()
    for i, (a, b) in enumerate(small):
        pltpu.make_async_copy(a, b, s_own.at[i]).start()
    for i in range(1, turns):
        fetch(i).start()

    def greet(where):
        pl.semaphore_signal(barrier, inc=1, device_id=where, device_id_type=MESH)

    greet(partner)
    greet(plane(za))

    @pl.when(mid)
    def _():
        greet(plane(zb))

    for j in range(1, side):
        greet({"ep": z * side + peer(j)})

    mine = part(core, half)
    loads = [
        (gw.at[0], wg), (uw.at[0], wu), (dw.at[0, :, part(core, span)], wd.at[mine]),
    ]
    for i, (a, b) in enumerate(loads):
        pltpu.make_async_copy(a, b, s_wl.at[i]).start()

    for i, (a, b) in enumerate(small):
        pltpu.make_async_copy(a, b, s_own.at[i]).wait()
    fold_at = tokens // 2
    facts = [ids[0:1].astype(jnp.float32), ids[1:2].astype(jnp.float32), rw[0:1], rw[1:2]]
    for i, fact in enumerate(facts):
        met[z, core, 2 * i : 2 * i + 1, :] = fact[:, :fold_at]
        met[z, core, 2 * i + 1 : 2 * i + 2, :] = fact[:, fold_at:]

    def lnorm(i):
        fetch(i).wait()
        at = part(i, slab)
        v = src[at, :].astype(jnp.float32)
        v = v - jnp.mean(v, axis=-1, keepdims=True)
        spread = jnp.mean(v * v, axis=-1, keepdims=True)
        y = v * lax.rsqrt(spread + 1e-05) * gain[...] + bias[...]
        y = y.astype(jnp.bfloat16)
        lo, hi = y[:, :span], y[:, span:]
        tok[z, core, at, :] = jnp.where(core == 0, lo, hi)
        oth[at, :] = jnp.where(core == 0, hi, lo)

    def waitbar():
        pl.semaphore_wait(barrier, side + 1 + jnp.where(mid, 1, 0))

    def lend(h):
        at = part(h, slab)
        remote(oth.at[at], tok.at[z, core, at], s_os.at[1], s_lent, partner)

    pl.loop(0, turns // 2)(lnorm)
    waitbar()
    remote(met.at[z, core], met.at[z, core], s_os.at[0], s_met.at[z, core], partner)
    pl.loop(0, turns // 2)(lend)

    @pl.loop(turns // 2, turns)
    def _(i):
        lnorm(i)
        lend(i)


    def send_tok(s, b, c, to, way):
        at = tok.at[s, b, :, cols(c)]
        remote(at, at, s_toks.at[way], s_tok.at[s, b, c], plane(to))

    def send_met(s, b, to, way):
        at = met.at[s, b]
        remote(at, at, s_mets.at[way], s_met.at[s, b], plane(to))

    def arrived(s, b, c):
        landed(tok.at[s, b, :, cols(c)], s_tok.at[s, b, c])

    def got_met(s, b):
        landed(met.at[s, b], s_met.at[s, b])

    def lent():
        landed(oth, s_lent)

    def own_tok(b, lo, hi):
        for c in range(lo, hi):
            send_tok(z, b, c, za, 0)

            if b == 0:
                @pl.when(mid)
                def _():
                    send_tok(z, b, c, zb, 1)

    def prep(q, b, s=None):
        s = order[q] if s is None else s
        ids0, ids1, wt0, wt1 = [
            jnp.concatenate([met[s, b, 2 * i : 2 * i + 1], met[s, b, 2 * i + 1 : 2 * i + 2]], axis=1)
            for i in range(4)
        ]
        row = lax.broadcasted_iota(jnp.int32, (rows, tokens), 0)
        e_row = (z * side + row // cap).astype(jnp.float32)
        s_row = lax.rem(row, cap).astype(jnp.float32)
        hit0 = (ids0 == e_row).astype(jnp.float32)
        hit1 = (ids1 == e_row).astype(jnp.float32)
        hit = hit0 + hit1
        before = (
            lax.broadcasted_iota(jnp.int32, (tokens, tokens), 0)
            < lax.broadcasted_iota(jnp.int32, (tokens, tokens), 1)
        ).astype(jnp.float32).astype(jnp.bfloat16)
        count = jnp.dot(hit.astype(jnp.bfloat16), before, preferred_element_type=jnp.float32)
        pick = jnp.where(count == s_row, hit, 0.0)
        sel[q, b] = pick.astype(jnp.bfloat16)
        w = (pick * (hit0 * wt0 + hit1 * wt1)).T
        high = w.astype(jnp.bfloat16)
        mix[q, b, 0] = high
        mix[q, b, 1] = (w - high.astype(jnp.float32)).astype(jnp.bfloat16)

    def disp(q, b, c, s=None):
        s = order[q] if s is None else s
        y = jnp.dot(sel[q, b], tok[s, b, :, cols(c)], preferred_element_type=jnp.float32)
        snd[q, b, :, cols(c)] = y.astype(jnp.bfloat16)
        xin[q, b, core, band(p), cols(c)] = snd[q, b, band(p), cols(c)]
        for j in range(1, side):
            o = peer(j)
            remote(
                snd.at[q, b, band(o), cols(c)], xin.at[q, b, core, band(p), cols(c)],
                s_xs, s_x.at[q, b, c], {"ep": z * side + o},
            )

    def others(ref):
        return ref.at[pl.ds(0, (side - 1) * cap)]

    def swap_x(q, b):
        @pl.loop(0, k)
        def _(c):
            at = xin.at[q, b, core, :, cols(c)]
            landed(others(at), s_x.at[q, b, c])
            remote(at, at, s_xds, s_xd.at[q, b], partner)

    tile = min(256, half)

    def gate(q, b):
        landed(xin.at[q, b, other], s_xd.at[q, b])

        @pl.loop(0, half // tile)
        def _(i):
            at = part(i, tile)
            lo, hi = xin[q, b, 0], xin[q, b, 1]
            g = jnp.dot(lo, wg[:span, at], preferred_element_type=jnp.float32)
            g = g + jnp.dot(hi, wg[span:, at], preferred_element_type=jnp.float32)
            u = jnp.dot(lo, wu[:span, at], preferred_element_type=jnp.float32)
            u = u + jnp.dot(hi, wu[span:, at], preferred_element_type=jnp.float32)
            v = g / (1.0 + jnp.exp(-g)) * u
            hid[q, b, core, :, at] = v.astype(jnp.bfloat16)
            done = hid.at[q, b, core, :, at]
            remote(done, done, s_hs, s_h.at[q, b], partner)

    def down(q, b, c):
        @pl.when(c == 0)
        def _():
            landed(hid.at[q, b, other], s_h.at[q, b])

        y = jnp.dot(hid[q, b, 0], wd[:half, cols(c)], preferred_element_type=jnp.float32)
        y = y + jnp.dot(hid[q, b, 1], wd[half:, cols(c)], preferred_element_type=jnp.float32)
        res[q, b, :, cols(c)] = y.astype(jnp.bfloat16)
        ret[q, b, band(p), cols(c)] = res[q, b, band(p), cols(c)]
        for j in range(1, side):
            o = peer(j)
            remote(
                res.at[q, b, band(o), cols(c)], ret.at[q, b, band(p), cols(c)],
                s_rs, s_r.at[q, b, c], {"ep": z * side + o},
            )

    def downs(q, b):
        pl.loop(0, k)(lambda c: down(q, b, c))

    def weigh(q, b, c):
        landed(others(ret.at[q, b, :, cols(c)]), s_r.at[q, b, c])
        r = ret[q, b, :, cols(c)]
        return jnp.dot(mix[q, b, 0], r, preferred_element_type=jnp.float32) + jnp.dot(
            mix[q, b, 1], r, preferred_element_type=jnp.float32
        )

    def combine(q, b, c, t, to, add):
        y = weigh(q, b, c)
        if add:
            landed(racc.at[t, b, c], s_p.at[t, b, c])
            y = y + racc[t, b, c].astype(jnp.float32)
        psend[q - 1, b, c] = y.astype(jnp.bfloat16)
        slot = jnp.where((to == t) & (to < z), n, t)
        remote(
            psend.at[q - 1, b, c], racc.at[slot, b, c], s_ps, s_p.at[slot, b, c], plane(to)
        )

    def weights():
        for i, (a, b) in enumerate(loads):
            pltpu.make_async_copy(a, b, s_wl.at[i]).wait()
        landed(wd.at[part(other, half)], s_wr)

    def own_met(b):
        send_met(z, b, za, 0)

        @pl.when(mid)
        def _():
            send_met(z, b, zb, 1)

    @pl.when(core == 0)
    def _():
        own_met(0)
        own_tok(0, 0, k)

    @pl.when(core == 1)
    def _():
        prep(0, 1)
        got_met(z, 0)
        own_met(0)
        lent()
        own_tok(0, 0, k)

    prep(0, 0)
    pl.loop(0, k)(lambda c: disp(0, 0, c))
    remote(dw.at[0, :, part(other, span)], wd.at[mine], s_ws, s_wr, partner)

    @pl.when(core == 0)
    def _():
        got_met(z, 1)
        lent()
        prep(0, 1)

    own_met(1)
    pl.when(end)(lambda: own_tok(1, 0, k))

    @pl.when(mid)
    def _():
        def relay(q, b, c):
            s = order[q]
            arrived(s, b, c)
            send_tok(s, b, c, za if q == 2 else zb, 0 if q == 2 else 1)

        def learn(q, b):
            got_met(order[q], b)
            send_met(order[q], b, za if q == 2 else zb, 0 if q == 2 else 1)
            prep(q, b)

        def fold(q, b, c):
            combine(q, b, c, order[q], zb if q == 2 else za, True)

        def folds(q, b, lo, hi):
            pl.loop(lo, hi)(lambda c: fold(q, b, c))

        learn(3, 0)
        learn(2, 0)

        @pl.loop(0, k)
        def _(c):
            relay(3, 0, c)
            relay(2, 0, c)
            disp(3, 0, c)
            disp(0, 1, c)

        learn(1, 0)
        learn(2, 1)

        @pl.loop(0, k)
        def _(c):
            relay(1, 0, c)
            relay(2, 1, c)
            disp(1, 0, c)
            disp(2, 0, c)

            @pl.when(c == 0)
            def _():
                weights()
                swap_x(0, 0)

            @pl.when(c == 1)
            def _():
                swap_x(3, 0)
                gate(0, 0)

            @pl.when(c == 2)
            def _():
                gate(3, 0)

        pl.loop(0, k)(lambda c: send_tok(z, 1, c, za, 0))
        learn(1, 1)

        @pl.loop(0, k)
        def _(c):
            relay(1, 1, c)
            disp(1, 1, c)
            down(3, 0, c)

            @pl.when(c == 1)
            def _():
                swap_x(0, 1)
                swap_x(1, 0)

            @pl.when(c == 2)
            def _():
                gate(1, 0)

        learn(3, 1)
        gate(0, 1)

        @pl.loop(0, k)
        def _(c):
            relay(3, 1, c)
            disp(3, 1, c)
            down(1, 0, c)

            @pl.when(c == 0)
            def _():
                swap_x(2, 0)

            @pl.when(c == 1)
            def _():
                swap_x(1, 1)
                gate(2, 0)

            @pl.when(c == 2)
            def _():
                gate(1, 1)

        pl.loop(0, k)(lambda c: send_tok(z, 1, c, zb, 1))
        pl.loop(0, k)(lambda c: disp(2, 1, c))
        folds(3, 0, 0, k)
        downs(1, 1)
        folds(1, 0, 0, k // 2)
        swap_x(3, 1)
        downs(2, 0)
        folds(1, 0, k // 2, k)
        swap_x(2, 1)
        gate(3, 1)
        downs(3, 1)
        gate(2, 1)

        @pl.loop(0, k // 2)
        def _(c):
            fold(1, 1, c)
            fold(2, 0, c)

        downs(2, 1)

        @pl.loop(k // 2, k)
        def _(c):
            fold(1, 1, c)
            fold(2, 0, c)

        downs(0, 0)

        @pl.loop(0, k // 2)
        def _(c):
            fold(3, 1, c)
            fold(2, 1, c)

        downs(0, 1)

        @pl.loop(k // 2, k)
        def _(c):
            fold(3, 1, c)
            fold(2, 1, c)

    @pl.when(end)
    def _():
        def take(q, b, c):
            s = z + (n - q) * step
            arrived(s, b, c)
            disp(q, b, c, s)

        def learn(q, b):
            s = z + (n - q) * step
            got_met(s, b)
            prep(q, b, s)

        def unit(i):
            return jnp.where(i < 3, 3 - i, i - 2), jnp.where(i < 3, 0, 1)

        def fold(q, b, c):
            combine(q, b, c, z + (n - q) * step, za, False)

        learn(3, 0)

        @pl.loop(0, k)
        def _(c):
            take(3, 0, c)

            @pl.when(c < k // 2)
            def _():
                disp(0, 1, c)

            @pl.when(c == 1)
            def _():
                weights()
                swap_x(0, 0)

            @pl.when(c == 2)
            def _():
                gate(0, 0)

        quarter = k // 4

        def piece(f, q, b, j, m=1):
            pl.loop(j * quarter, (j + m) * quarter)(lambda c: f(q, b, c))

        piece(disp, 0, 1, 2, 2)
        piece(down, 0, 0, 0)
        learn(2, 0)
        swap_x(3, 0)
        piece(take, 2, 0, 0)
        gate(3, 0)
        piece(take, 2, 0, 1)
        piece(down, 3, 0, 0, 2)
        piece(take, 2, 0, 2)
        piece(take, 2, 0, 3)
        piece(down, 3, 0, 2, 2)
        piece(fold, 3, 0, 0)

        @pl.loop(1, 5)
        def _(i):
            q, b = unit(i)
            q1, b1 = unit(i + 1)
            q0, b0 = unit(i - 1)
            learn(q1, b1)
            piece(take, q1, b1, 0)
            piece(fold, q0, b0, 1)
            swap_x(q, b)
            piece(take, q1, b1, 1)
            gate(q, b)
            piece(fold, q0, b0, 2)
            piece(take, q1, b1, 2)
            piece(down, q, b, 0, 2)
            piece(fold, q0, b0, 3)
            piece(take, q1, b1, 3)
            piece(down, q, b, 2, 2)

            @pl.when(i == 1)
            def _():
                swap_x(0, 1)

            @pl.when(i == 2)
            def _():
                gate(0, 1)

            @pl.when(i == 4)
            def _():
                piece(down, 0, 1, 0, 3)

            piece(fold, q, b, 0)

        swap_x(3, 1)
        piece(fold, 2, 1, 1)
        gate(3, 1)
        piece(fold, 2, 1, 2, 2)
        downs(3, 1)
        piece(down, 0, 0, 1, 3)
        piece(down, 0, 1, 3)
        piece(fold, 3, 1, 0, 4)

    def last(b, c, slots):
        y = weigh(0, b, c)
        for slot in slots:
            landed(racc.at[slot, b, c], s_p.at[slot, b, c])
            y = y + racc[slot, b, c].astype(jnp.float32)
        to = pl.ds(pl.multiple_of(core * span + c * wide, wide), wide)

        @pl.when(core == b)
        def _():
            out[:, to] = y.astype(out.dtype)

        @pl.when(core != b)
        def _():
            obuf[c] = y.astype(out.dtype)
            remote(obuf.at[c], out.at[:, to], s_od, s_or, partner)

    @pl.when(end)
    def _():
        for b in range(2):
            pl.loop(0, k)(lambda c: last(b, c, [jnp.where(z == 0, n, z)]))

    @pl.when(mid)
    def _():
        for b in range(2):
            pl.loop(0, k)(lambda c: last(b, c, [z, n]))

    drain = landed
    drain(met.at[z, core], s_os.at[0])
    drain(oth, s_os.at[1])
    drain(wd.at[mine], s_ws)
    sent = pl.ds(0, (side - 1) * cap)

    @pl.when(end)
    def _():
        drain(tok.at[0], s_toks.at[0])
        drain(met.at[0], s_mets.at[0])

    @pl.when(mid)
    def _():
        for way in range(2):
            drain(tok.at[pl.ds(0, 2 + way)], s_toks.at[way])
            drain(met.at[pl.ds(0, 2 + way)], s_mets.at[way])

    drain(snd.at[:, :, sent], s_xs)
    drain(res.at[:, :, sent], s_rs)
    drain(snd, s_xds)
    drain(hid.at[:, :, 0], s_hs)
    drain(psend, s_ps)
    drain(obuf, s_od)
    drain(obuf, s_or)


def body(
    tokens, norm_gain, norm_bias, gate_weight, up_weight, down_weight, expert_ids, route_weights
):
    count, width = tokens.shape
    experts = lax.axis_size("ep")
    cap = max(4 * count // experts, 4)
    side = experts // LINE
    half = gate_weight.shape[2]
    rows = side * cap
    span = width // 2
    wide = span // CHUNKS
    bf = jnp.bfloat16
    dma = pltpu.SemaphoreType.DMA
    hbm = pl.BlockSpec(memory_space=pl.ANY)
    return pl.pallas_call(
        functools.partial(kernel, side),
        out_shape=pltpu.VMEM((count, width), bf),
        in_specs=[hbm] * 8,
        out_specs=pl.BlockSpec(memory_space=pltpu.VMEM),
        scratch_shapes=[
            pltpu.VMEM((count, width), bf),
            pltpu.VMEM((1, width), jnp.float32),
            pltpu.VMEM((1, width), jnp.float32),
            pltpu.VMEM((2, count), jnp.int32),
            pltpu.VMEM((2, count), jnp.float32),
            pltpu.VMEM((count, span), bf),
            pltpu.VMEM((LINE, 2, count, span), bf),
            pltpu.VMEM((LINE, 2, 8, count // 2), jnp.float32),
            pltpu.VMEM((width, half), bf),
            pltpu.VMEM((width, half), bf),
            pltpu.VMEM((2 * half, span), bf),
            pltpu.VMEM((LINE, 2, rows, count), bf),
            pltpu.VMEM((LINE, 2, 2, count, rows), bf),
            pltpu.VMEM((LINE, 2, rows, span), bf),
            pltpu.VMEM((LINE, 2, 2, rows, span), bf),
            pltpu.VMEM((LINE, 2, 2, rows, half), bf),
            pltpu.VMEM((LINE, 2, rows, span), bf),
            pltpu.VMEM((LINE, 2, rows, span), bf),
            pltpu.VMEM((LINE - 1, 2, CHUNKS, count, wide), bf),
            pltpu.VMEM((LINE + 1, 2, CHUNKS, count, wide), bf),
            pltpu.VMEM((CHUNKS, count, wide), bf),
            dma((4 + count // min(64, count),)),
            dma,
            dma((3,)),
            dma,
            dma,
            dma((LINE, 2, CHUNKS)),
            dma((2,)),
            dma((LINE, 2)),
            dma((2,)),
            dma((2,)),
            dma((LINE, 2, CHUNKS)),
            dma,
            dma((LINE, 2)),
            dma,
            dma((LINE, 2)),
            dma,
            dma((LINE, 2, CHUNKS)),
            dma,
            dma((LINE + 1, 2, CHUNKS)),
            dma,
            dma,
            dma,
        ],
        compiler_params=pltpu.CompilerParams(
            collective_id=0, has_side_effects=True, vmem_limit_bytes=56 * 1024 * 1024
        ),
    )(
        tokens, norm_gain[None], norm_bias[None], expert_ids.T, route_weights.T,
        gate_weight, up_weight, down_weight,
    )


def solution(mesh):
    placed = (
        P(("ep", "tp"), None),
        P(),
        P(),
        P("ep", None, "tp"),
        P("ep", None, "tp"),
        P("ep", "tp", None),
        P(("ep", "tp"), None),
        P(("ep", "tp"), None),
    )
    return jax.shard_map(
        body, mesh=mesh, in_specs=placed, out_specs=P(("ep", "tp"), None), check_vma=False
    )
```

```python
import functools

import jax
import jax.numpy as jnp
from jax import lax
from jax.experimental import pallas as pl
from jax.experimental.pallas import tpu as pltpu
from jax.sharding import PartitionSpec as P

MESH = pl.DeviceIdType.MESH
LINE = 4
CHUNKS = 4


def kernel(
    planes, raw, gain_in, bias_in, ids_in, rw_in, gw, uw, dw, out,
    src, gain, bias, ids, rw, oth, tok, met, wg, wu, wd, sel, mix, snd, xin, hid, res, ret, psend, racc, home,
    s_own, s_lent, s_wl, s_ws, s_wr, s_tok, s_toks, s_met, s_mets, s_os, s_x, s_xs, s_xd, s_xds,
    s_h, s_hs, s_r, s_rs, s_p, s_ps, s_home, s_rd,
):
    n = LINE
    side = planes
    me, core = lax.axis_index("ep"), lax.axis_index("tp")
    other = 1 - core
    z, p = me // side, lax.rem(me, side)
    tokens, width = raw.shape
    half = gw.shape[2]
    span = width // 2
    rows = snd.shape[2]
    cap = rows // side
    k = CHUNKS
    wide = span // k
    end = (z == 0) | (z == n - 1)
    mid = jnp.logical_not(end)
    step = jnp.where(z < n // 2, 1, -1)
    za, zb = z + step, z - step
    order = [
        z,
        jnp.where(end, z + 3 * step, z + 2 * step),
        jnp.where(end, z + 2 * step, z - step),
        z + step,
    ]

    def cols(c):
        return pl.ds(pl.multiple_of(c * wide, wide), wide)

    def part(h, size):
        return pl.ds(pl.multiple_of(h * size, size), size)

    def band(i):
        return pl.ds(pl.multiple_of(i * cap, cap), cap)

    def plane(t):
        return {"ep": t * side + p}

    partner = {"tp": other}

    def peer(j):
        return lax.rem(p + j, side)

    def remote(src, dst, send, recv, where):
        pltpu.make_async_remote_copy(
            src_ref=src, dst_ref=dst, send_sem=send, recv_sem=recv,
            device_id=where, device_id_type=MESH,
        ).start()

    def landed(ref, sem):
        pltpu.make_async_copy(ref, ref, sem).wait()

    barrier = pltpu.get_barrier_semaphore()
    small = [(ids_in, ids), (rw_in, rw), (gain_in, gain), (bias_in, bias)]
    slab = min(64, tokens)
    turns = tokens // slab

    def fetch(i):
        at = part(i, slab)
        return pltpu.make_async_copy(raw.at[at], src.at[at], s_own.at[len(small) + i])

    fetch(0).start()
    for i, (a, b) in enumerate(small):
        pltpu.make_async_copy(a, b, s_own.at[i]).start()
    for i in range(1, turns):
        fetch(i).start()

    def greet(where):
        pl.semaphore_signal(barrier, inc=1, device_id=where, device_id_type=MESH)

    for twin in range(2):
        greet({"ep": za * side + p, "tp": twin})

        @pl.when(mid)
        def _():
            greet({"ep": zb * side + p, "tp": twin})

        for j in range(1, side):
            greet({"ep": z * side + peer(j), "tp": twin})

    greet(partner)
    mine = part(core, half)
    loads = [
        (gw.at[0], wg), (uw.at[0], wu), (dw.at[0, :, part(core, span)], wd.at[mine]),
    ]
    for i, (a, b) in enumerate(loads):
        pltpu.make_async_copy(a, b, s_wl.at[i]).start()

    for i, (a, b) in enumerate(small):
        pltpu.make_async_copy(a, b, s_own.at[i]).wait()
    fold_at = tokens // 2
    facts = [ids[0:1].astype(jnp.float32), ids[1:2].astype(jnp.float32), rw[0:1], rw[1:2]]
    for i, fact in enumerate(facts):
        met[z, core, 2 * i : 2 * i + 1, :] = fact[:, :fold_at]
        met[z, core, 2 * i + 1 : 2 * i + 2, :] = fact[:, fold_at:]

    def lnorm(i):
        fetch(i).wait()
        at = part(i, slab)
        v = src[at, :].astype(jnp.float32)
        v = v - jnp.mean(v, axis=-1, keepdims=True)
        spread = jnp.mean(v * v, axis=-1, keepdims=True)
        y = v * lax.rsqrt(spread + 1e-05) * gain[...] + bias[...]
        y = y.astype(jnp.bfloat16)
        lo, hi = y[:, :span], y[:, span:]
        tok[z, core, at, :] = jnp.where(core == 0, lo, hi)
        oth[at, :] = jnp.where(core == 0, hi, lo)

    def waitbar():
        pl.semaphore_wait(barrier, 2 * side + 1 + jnp.where(mid, 2, 0))

    def lend(h):
        at = part(h, slab)
        remote(oth.at[at], tok.at[z, core, at], s_os.at[1], s_lent, partner)

    pl.loop(0, turns // 2)(lnorm)
    waitbar()
    remote(met.at[z, core], met.at[z, core], s_os.at[0], s_met.at[z, core], partner)
    pl.loop(0, turns // 2)(lend)

    @pl.loop(turns // 2, turns)
    def _(i):
        lnorm(i)
        lend(i)


    def send_tok(s, b, c, to, way, place):
        at = tok.at[s, b, :, cols(c)]
        remote(at, at, s_toks.at[way], s_tok.at[place - 1, b, c], plane(to))

    def send_met(s, b, to, way):
        at = met.at[s, b]
        remote(at, at, s_mets.at[way], s_met.at[s, b], plane(to))

    def arrived(q, s, b, c):
        landed(tok.at[s, b, :, cols(c)], s_tok.at[q - 1, b, c])

    def got_met(s, b):
        landed(met.at[s, b], s_met.at[s, b])

    def lent():
        landed(oth, s_lent)

    def own_tok(b, lo, hi):
        for c in range(lo, hi):
            send_tok(z, b, c, za, 0, jnp.where(end, 2, 3))

            if b == 0:
                @pl.when(mid)
                def _():
                    send_tok(z, b, c, zb, 1, 3)

    def prep(q, b, s=None):
        s = order[q] if s is None else s
        ids0, ids1, wt0, wt1 = [
            jnp.concatenate([met[s, b, 2 * i : 2 * i + 1], met[s, b, 2 * i + 1 : 2 * i + 2]], axis=1)
            for i in range(4)
        ]
        row = lax.broadcasted_iota(jnp.int32, (rows, tokens), 0)
        e_row = (z * side + row // cap).astype(jnp.float32)
        s_row = lax.rem(row, cap).astype(jnp.float32)
        hit0 = (ids0 == e_row).astype(jnp.float32)
        hit1 = (ids1 == e_row).astype(jnp.float32)
        hit = hit0 + hit1
        before = (
            lax.broadcasted_iota(jnp.int32, (tokens, tokens), 0)
            < lax.broadcasted_iota(jnp.int32, (tokens, tokens), 1)
        ).astype(jnp.float32).astype(jnp.bfloat16)
        count = jnp.dot(hit.astype(jnp.bfloat16), before, preferred_element_type=jnp.float32)
        pick = jnp.where(count == s_row, hit, 0.0)
        sel[q, b] = pick.astype(jnp.bfloat16)
        w = (pick * (hit0 * wt0 + hit1 * wt1)).T
        high = w.astype(jnp.bfloat16)
        mix[q, b, 0] = high
        mix[q, b, 1] = (w - high.astype(jnp.float32)).astype(jnp.bfloat16)

    def disp(q, b, c, s=None):
        s = order[q] if s is None else s
        y = jnp.dot(sel[q, b], tok[s, b, :, cols(c)], preferred_element_type=jnp.float32)
        snd[q, b, :, cols(c)] = y.astype(jnp.bfloat16)
        xin[q, b, core, band(p), cols(c)] = snd[q, b, band(p), cols(c)]
        for j in range(1, side):
            o = peer(j)
            remote(
                snd.at[q, b, band(o), cols(c)], xin.at[q, b, core, band(p), cols(c)],
                s_xs, s_x.at[q, b, c], {"ep": z * side + o},
            )

    def others(ref):
        return ref.at[pl.ds(0, (side - 1) * cap)]

    def swap_x(q, b):
        @pl.loop(0, k)
        def _(c):
            at = xin.at[q, b, core, :, cols(c)]
            landed(others(at), s_x.at[q, b, c])
            remote(at, at, s_xds, s_xd.at[q, b], partner)

    tile = min(256, half)

    def gate(q, b):
        landed(xin.at[q, b, other], s_xd.at[q, b])

        @pl.loop(0, half // tile)
        def _(i):
            at = part(i, tile)
            lo, hi = xin[q, b, 0], xin[q, b, 1]
            g = jnp.dot(lo, wg[:span, at], preferred_element_type=jnp.float32)
            g = g + jnp.dot(hi, wg[span:, at], preferred_element_type=jnp.float32)
            u = jnp.dot(lo, wu[:span, at], preferred_element_type=jnp.float32)
            u = u + jnp.dot(hi, wu[span:, at], preferred_element_type=jnp.float32)
            v = g / (1.0 + jnp.exp(-g)) * u
            hid[q, b, core, :, at] = v.astype(jnp.bfloat16)
            done = hid.at[q, b, core, :, at]
            remote(done, done, s_hs, s_h.at[q, b], partner)

    def down(q, b, c):
        @pl.when(c == 0)
        def _():
            landed(hid.at[q, b, other], s_h.at[q, b])

        y = jnp.dot(hid[q, b, 0], wd[:half, cols(c)], preferred_element_type=jnp.float32)
        y = y + jnp.dot(hid[q, b, 1], wd[half:, cols(c)], preferred_element_type=jnp.float32)
        res[q, b, :, cols(c)] = y.astype(jnp.bfloat16)
        yours = isinstance(q, int) and q == 0
        slot = core if yours else b
        at = ret.at[q, slot, band(p), cols(c)]

        def keep():
            ret[q, slot, band(p), cols(c)] = res[q, b, band(p), cols(c)]

        if yours:
            pl.when(core == b)(keep)

            @pl.when(core != b)
            def _():
                remote(res.at[q, b, band(p), cols(c)], at, s_rd, s_r.at[q, slot, c], partner)
        else:
            keep()
        for j in range(1, side):
            o = peer(j)
            where = {"ep": z * side + o, "tp": b} if yours else {"ep": z * side + o}
            remote(res.at[q, b, band(o), cols(c)], at, s_rs, s_r.at[q, slot, c], where)

    def downs(q, b):
        pl.loop(0, k)(lambda c: down(q, b, c))

    def mixed(q, b, r):
        return jnp.dot(mix[q, b, 0], r, preferred_element_type=jnp.float32) + jnp.dot(
            mix[q, b, 1], r, preferred_element_type=jnp.float32
        )

    def combine(q, b, c, t, to, add):
        landed(others(ret.at[q, b, :, cols(c)]), s_r.at[q, b, c])
        y = mixed(q, b, ret[q, b, :, cols(c)])
        if add:
            landed(racc.at[q - 1, b, c], s_p.at[q - 1, b, c])
            y = y + racc[q - 1, b, c].astype(jnp.float32)
        psend[q - 1, b, c] = y.astype(jnp.bfloat16)
        theirs = to == t

        @pl.when(theirs)
        def _():
            way = jnp.where(end, 1, 0)
            remote(
                psend.at[q - 1, b, c], home.at[way, core, c], s_ps, s_home.at[way, core, c],
                {"ep": to * side + p, "tp": b},
            )

        @pl.when(jnp.logical_not(theirs))
        def _():
            slot = jnp.where(end, jnp.where(q == 1, 0, 2), 1)
            remote(
                psend.at[q - 1, b, c], racc.at[slot, b, c], s_ps, s_p.at[slot, b, c], plane(to)
            )

    def weights():
        for i, (a, b) in enumerate(loads):
            pltpu.make_async_copy(a, b, s_wl.at[i]).wait()
        landed(wd.at[part(other, half)], s_wr)

    def own_met(b):
        send_met(z, b, za, 0)

        @pl.when(mid)
        def _():
            send_met(z, b, zb, 1)

    @pl.when(core == 0)
    def _():
        own_met(0)
        own_tok(0, 0, k)

    @pl.when(core == 1)
    def _():
        prep(0, 1)
        disp(0, 1, 0)
        got_met(z, 0)
        own_met(0)
        lent()
        own_tok(0, 0, k)

    prep(0, 0)
    pl.loop(0, k)(lambda c: disp(0, 0, c))
    remote(dw.at[0, :, part(other, span)], wd.at[mine], s_ws, s_wr, partner)

    @pl.when(core == 0)
    def _():
        got_met(z, 1)
        lent()
        prep(0, 1)

    own_met(1)
    def spare(c):
        @pl.when((core == 0) | (c > 0))
        def _():
            disp(0, 1, c)

    pl.when(end)(lambda: own_tok(1, 0, k))

    @pl.when(mid)
    def _():
        def relay(q, b, c):
            s = order[q]
            arrived(q, s, b, c)
            send_tok(s, b, c, za if q == 2 else zb, 0 if q == 2 else 1, 2 if q == 3 else 1)

        def learn(q, b):
            got_met(order[q], b)
            send_met(order[q], b, za if q == 2 else zb, 0 if q == 2 else 1)
            prep(q, b)

        def fold(q, b, c):
            combine(q, b, c, order[q], zb if q == 2 else za, True)

        def folds(q, b, lo, hi):
            pl.loop(lo, hi)(lambda c: fold(q, b, c))

        learn(3, 0)
        learn(2, 0)

        @pl.loop(0, k)
        def _(c):
            relay(3, 0, c)
            relay(2, 0, c)
            disp(3, 0, c)
            spare(c)

        learn(1, 0)
        learn(2, 1)

        @pl.loop(0, k)
        def _(c):
            relay(1, 0, c)
            relay(2, 1, c)
            disp(1, 0, c)
            disp(2, 0, c)

            @pl.when(c == 0)
            def _():
                weights()
                swap_x(0, 0)

            @pl.when(c == 1)
            def _():
                swap_x(3, 0)
                gate(0, 0)

            @pl.when(c == 2)
            def _():
                gate(3, 0)

        pl.loop(0, k)(lambda c: send_tok(z, 1, c, za, 0, 3))
        learn(1, 1)

        @pl.loop(0, k)
        def _(c):
            relay(1, 1, c)
            disp(1, 1, c)
            down(3, 0, c)

            @pl.when(c == 1)
            def _():
                swap_x(0, 1)
                swap_x(1, 0)

            @pl.when(c == 2)
            def _():
                gate(1, 0)

        learn(3, 1)
        gate(0, 1)

        @pl.loop(0, k)
        def _(c):
            relay(3, 1, c)
            disp(3, 1, c)
            down(1, 0, c)

            @pl.when(c == 0)
            def _():
                swap_x(2, 0)

            @pl.when(c == 1)
            def _():
                swap_x(1, 1)
                gate(2, 0)

            @pl.when(c == 2)
            def _():
                gate(1, 1)

        pl.loop(0, k)(lambda c: send_tok(z, 1, c, zb, 1, 3))
        pl.loop(0, k)(lambda c: disp(2, 1, c))
        folds(3, 0, 0, k)
        downs(1, 1)
        folds(1, 0, 0, k // 2)
        swap_x(3, 1)
        downs(2, 0)
        folds(1, 0, k // 2, k)
        swap_x(2, 1)
        gate(3, 1)
        downs(3, 1)
        gate(2, 1)

        @pl.loop(0, k // 2)
        def _(c):
            fold(1, 1, c)
            fold(2, 0, c)

        downs(2, 1)

        @pl.loop(k // 2, k)
        def _(c):
            fold(1, 1, c)
            fold(2, 0, c)

        downs(0, 0)

        @pl.loop(0, k // 2)
        def _(c):
            fold(3, 1, c)
            fold(2, 1, c)

        downs(0, 1)

        @pl.loop(k // 2, k)
        def _(c):
            fold(3, 1, c)
            fold(2, 1, c)

    @pl.when(end)
    def _():
        def take(q, b, c):
            s = z + (n - q) * step
            arrived(q, s, b, c)
            disp(q, b, c, s)

        def learn(q, b):
            s = z + (n - q) * step
            got_met(s, b)
            prep(q, b, s)

        def unit(i):
            return jnp.where(i < 3, 3 - i, i - 2), jnp.where(i < 3, 0, 1)

        def fold(q, b, c):
            combine(q, b, c, z + (n - q) * step, za, False)

        learn(3, 0)

        @pl.loop(0, k)
        def _(c):
            take(3, 0, c)

            @pl.when(c < k // 2)
            def _():
                spare(c)

            @pl.when(c == 1)
            def _():
                weights()
                swap_x(0, 0)

            @pl.when(c == 2)
            def _():
                gate(0, 0)

        quarter = k // 4

        def piece(f, q, b, j, m=1):
            pl.loop(j * quarter, (j + m) * quarter)(lambda c: f(q, b, c))

        piece(disp, 0, 1, 2, 2)
        learn(2, 0)
        swap_x(3, 0)
        piece(take, 2, 0, 0)
        gate(3, 0)
        piece(take, 2, 0, 1)
        piece(down, 3, 0, 0, 2)
        piece(take, 2, 0, 2)
        piece(take, 2, 0, 3)
        piece(down, 3, 0, 2, 2)
        piece(fold, 3, 0, 0)

        @pl.loop(1, 5)
        def _(i):
            q, b = unit(i)
            q1, b1 = unit(i + 1)
            q0, b0 = unit(i - 1)
            learn(q1, b1)
            piece(take, q1, b1, 0)
            piece(fold, q0, b0, 1)
            swap_x(q, b)
            piece(take, q1, b1, 1)
            gate(q, b)
            piece(fold, q0, b0, 2)
            piece(take, q1, b1, 2)
            piece(down, q, b, 0, 2)
            piece(fold, q0, b0, 3)
            piece(take, q1, b1, 3)
            piece(down, q, b, 2, 2)

            @pl.when(i == 1)
            def _():
                swap_x(0, 1)

            @pl.when(i == 2)
            def _():
                gate(0, 1)

            @pl.when(i == 4)
            def _():
                piece(down, 0, 1, 0, 3)

            piece(fold, q, b, 0)

        swap_x(3, 1)
        piece(fold, 2, 1, 1)
        gate(3, 1)
        piece(fold, 2, 1, 2, 2)
        downs(3, 1)
        downs(0, 0)
        piece(down, 0, 1, 3)
        piece(fold, 3, 1, 0, 4)

    def last(h, c, ways):
        at = ret.at[0, h, :, cols(c)]
        pl.when(core == h)(lambda: landed(others(at), s_r.at[0, h, c]))
        pl.when(core != h)(lambda: landed(at, s_r.at[0, h, c]))
        y = mixed(0, core, at[...])
        for way in ways:
            landed(home.at[way, h, c], s_home.at[way, h, c])
            y = y + home[way, h, c].astype(jnp.float32)
        out[:, pl.ds(pl.multiple_of(h * span + c * wide, wide), wide)] = y.astype(out.dtype)

    @pl.when(end)
    def _():
        @pl.loop(0, k)
        def _(c):
            last(0, c, [0])
            last(1, c, [0])

    @pl.when(mid)
    def _():
        @pl.loop(0, k)
        def _(c):
            last(0, c, [0, 1])
            last(1, c, [0, 1])

    drain = landed
    drain(met.at[z, core], s_os.at[0])
    drain(oth, s_os.at[1])
    drain(wd.at[mine], s_ws)
    sent = pl.ds(0, (side - 1) * cap)

    @pl.when(end)
    def _():
        drain(tok.at[0], s_toks.at[0])
        drain(met.at[0], s_mets.at[0])

    @pl.when(mid)
    def _():
        for way in range(2):
            drain(tok.at[pl.ds(0, 2 + way)], s_toks.at[way])
            drain(met.at[pl.ds(0, 2 + way)], s_mets.at[way])

    drain(snd.at[:, :, sent], s_xs)
    drain(res.at[:, :, sent], s_rs)
    drain(snd, s_xds)
    drain(hid.at[:, :, 0], s_hs)
    drain(psend, s_ps)
    drain(res.at[0, 0, pl.ds(0, cap)], s_rd)


def body(
    tokens, norm_gain, norm_bias, gate_weight, up_weight, down_weight, expert_ids, route_weights
):
    count, width = tokens.shape
    experts = lax.axis_size("ep")
    cap = max(4 * count // experts, 4)
    side = experts // LINE
    half = gate_weight.shape[2]
    rows = side * cap
    span = width // 2
    wide = span // CHUNKS
    bf = jnp.bfloat16
    dma = pltpu.SemaphoreType.DMA
    hbm = pl.BlockSpec(memory_space=pl.ANY)
    return pl.pallas_call(
        functools.partial(kernel, side),
        out_shape=pltpu.VMEM((count, width), bf),
        in_specs=[hbm] * 8,
        out_specs=pl.BlockSpec(memory_space=pltpu.VMEM),
        scratch_shapes=[
            pltpu.VMEM((count, width), bf),
            pltpu.VMEM((1, width), jnp.float32),
            pltpu.VMEM((1, width), jnp.float32),
            pltpu.VMEM((2, count), jnp.int32),
            pltpu.VMEM((2, count), jnp.float32),
            pltpu.VMEM((count, span), bf),
            pltpu.VMEM((LINE, 2, count, span), bf),
            pltpu.VMEM((LINE, 2, 8, count // 2), jnp.float32),
            pltpu.VMEM((width, half), bf),
            pltpu.VMEM((width, half), bf),
            pltpu.VMEM((2 * half, span), bf),
            pltpu.VMEM((LINE, 2, rows, count), bf),
            pltpu.VMEM((LINE, 2, 2, count, rows), bf),
            pltpu.VMEM((LINE, 2, rows, span), bf),
            pltpu.VMEM((LINE, 2, 2, rows, span), bf),
            pltpu.VMEM((LINE, 2, 2, rows, half), bf),
            pltpu.VMEM((LINE, 2, rows, span), bf),
            pltpu.VMEM((LINE, 2, rows, span), bf),
            pltpu.VMEM((LINE - 1, 2, CHUNKS, count, wide), bf),
            pltpu.VMEM((LINE - 1, 2, CHUNKS, count, wide), bf),
            pltpu.VMEM((2, 2, CHUNKS, count, wide), bf),
            dma((4 + count // min(64, count),)),
            dma,
            dma((3,)),
            dma,
            dma,
            dma((LINE - 1, 2, CHUNKS)),
            dma((2,)),
            dma((LINE, 2)),
            dma((2,)),
            dma((2,)),
            dma((LINE, 2, CHUNKS)),
            dma,
            dma((LINE, 2)),
            dma,
            dma((LINE, 2)),
            dma,
            dma((LINE, 2, CHUNKS)),
            dma,
            dma((LINE - 1, 2, CHUNKS)),
            dma,
            dma((2, 2, CHUNKS)),
            dma,
        ],
        compiler_params=pltpu.CompilerParams(
            collective_id=0, has_side_effects=True, vmem_limit_bytes=56 * 1024 * 1024
        ),
    )(
        tokens, norm_gain[None], norm_bias[None], expert_ids.T, route_weights.T,
        gate_weight, up_weight, down_weight,
    )


def solution(mesh):
    placed = (
        P(("ep", "tp"), None),
        P(),
        P(),
        P("ep", None, "tp"),
        P("ep", None, "tp"),
        P("ep", "tp", None),
        P(("ep", "tp"), None),
        P(("ep", "tp"), None),
    )
    return jax.shard_map(
        body, mesh=mesh, in_specs=placed, out_specs=P(("ep", "tp"), None), check_vma=False
    )
```

```python
import functools

import jax
import jax.numpy as jnp
from jax import lax
from jax.experimental import pallas as pl
from jax.experimental.pallas import tpu as pltpu
from jax.sharding import PartitionSpec as P

MESH = pl.DeviceIdType.MESH
LINE = 4
CHUNKS = 4


def kernel(
    planes, raw, gain_in, bias_in, ids_in, rw_in, gw, uw, dw, out,
    src, gain, bias, ids, rw, oth, tok, met, wg, wu, wd, sel, mix, snd, xin, hid, res, ret, psend, racc, home,
    s_own, s_lent, s_wl, s_ws, s_wr, s_tok, s_toks, s_met, s_mets, s_os, s_x, s_xs, s_xd, s_xds,
    s_h, s_hs, s_r, s_rs, s_p, s_ps, s_home, s_rd,
):
    n = LINE
    side = planes
    me, core = lax.axis_index("ep"), lax.axis_index("tp")
    other = 1 - core
    z, p = me // side, lax.rem(me, side)
    tokens, width = raw.shape
    half = gw.shape[2]
    span = width // 2
    rows = snd.shape[2]
    cap = rows // side
    k = CHUNKS
    wide = span // k
    end = (z == 0) | (z == n - 1)
    mid = jnp.logical_not(end)
    step = jnp.where(z < n // 2, 1, -1)
    za, zb = z + step, z - step
    order = [
        z,
        jnp.where(end, z + 3 * step, z + 2 * step),
        jnp.where(end, z + 2 * step, z - step),
        z + step,
    ]

    def cols(c):
        return pl.ds(pl.multiple_of(c * wide, wide), wide)

    def part(h, size):
        return pl.ds(pl.multiple_of(h * size, size), size)

    def band(i):
        return pl.ds(pl.multiple_of(i * cap, cap), cap)

    def plane(t):
        return {"ep": t * side + p}

    partner = {"tp": other}

    def peer(j):
        return lax.rem(p + j, side)

    def remote(src, dst, send, recv, where):
        pltpu.make_async_remote_copy(
            src_ref=src, dst_ref=dst, send_sem=send, recv_sem=recv,
            device_id=where, device_id_type=MESH,
        ).start()

    def landed(ref, sem):
        pltpu.make_async_copy(ref, ref, sem).wait()

    barrier = pltpu.get_barrier_semaphore()
    small = [(ids_in, ids), (rw_in, rw), (gain_in, gain), (bias_in, bias)]
    slab = min(64, tokens)
    turns = tokens // slab

    def fetch(i):
        at = part(i, slab)
        return pltpu.make_async_copy(raw.at[at], src.at[at], s_own.at[len(small) + i])

    fetch(0).start()
    for i, (a, b) in enumerate(small):
        pltpu.make_async_copy(a, b, s_own.at[i]).start()
    for i in range(1, turns):
        fetch(i).start()

    def greet(where):
        pl.semaphore_signal(barrier, inc=1, device_id=where, device_id_type=MESH)

    for twin in range(2):
        greet({"ep": za * side + p, "tp": twin})

        @pl.when(mid)
        def _():
            greet({"ep": zb * side + p, "tp": twin})

        for j in range(1, side):
            greet({"ep": z * side + peer(j), "tp": twin})

    greet(partner)
    mine = part(core, half)
    loads = [
        (gw.at[0], wg), (uw.at[0], wu), (dw.at[0, :, part(core, span)], wd.at[mine]),
    ]
    for i, (a, b) in enumerate(loads):
        pltpu.make_async_copy(a, b, s_wl.at[i]).start()

    for i, (a, b) in enumerate(small):
        pltpu.make_async_copy(a, b, s_own.at[i]).wait()
    fold_at = tokens // 2
    facts = [ids[0:1].astype(jnp.float32), ids[1:2].astype(jnp.float32), rw[0:1], rw[1:2]]
    for i, fact in enumerate(facts):
        met[z, core, 2 * i : 2 * i + 1, :] = fact[:, :fold_at]
        met[z, core, 2 * i + 1 : 2 * i + 2, :] = fact[:, fold_at:]

    def lnorm(i):
        fetch(i).wait()
        at = part(i, slab)
        v = src[at, :].astype(jnp.float32)
        v = v - jnp.mean(v, axis=-1, keepdims=True)
        spread = jnp.mean(v * v, axis=-1, keepdims=True)
        y = v * lax.rsqrt(spread + 1e-05) * gain[...] + bias[...]
        y = y.astype(jnp.bfloat16)
        lo, hi = y[:, :span], y[:, span:]
        tok[z, core, at, :] = jnp.where(core == 0, lo, hi)
        oth[at, :] = jnp.where(core == 0, hi, lo)

    def waitbar():
        pl.semaphore_wait(barrier, 2 * side + 1 + jnp.where(mid, 2, 0))

    def lend(h):
        at = part(h, slab)
        remote(oth.at[at], tok.at[z, core, at], s_os.at[1], s_lent.at[h // (turns // 2)], partner)

    pl.loop(0, turns // 2)(lnorm)
    waitbar()
    remote(met.at[z, core], met.at[z, core], s_os.at[0], s_met.at[z, core], partner)
    pl.loop(0, turns // 2)(lend)

    @pl.loop(turns // 2, turns)
    def _(i):
        lnorm(i)
        lend(i)


    def send_tok(s, b, c, to, way, place):
        at = tok.at[s, b, :, cols(c)]
        remote(at, at, s_toks.at[way], s_tok.at[place - 1, b, c], plane(to))

    def send_met(s, b, to, way):
        at = met.at[s, b]
        remote(at, at, s_mets.at[way], s_met.at[s, b], plane(to))

    def arrived(q, s, b, c):
        landed(tok.at[s, b, :, cols(c)], s_tok.at[q - 1, b, c])

    def got_met(s, b):
        landed(met.at[s, b], s_met.at[s, b])

    def lent():
        for h in range(2):
            landed(oth.at[part(h, tokens // 2)], s_lent.at[h])

    def send_part(at, c, to, way, place):
        piece_at = tok.at[z, 0, at, cols(c)]
        remote(piece_at, piece_at, s_toks.at[way], s_tok.at[place - 1, 0, c], plane(to))

    def own_tok(b, lo, hi):
        for c in range(lo, hi):
            send_tok(z, b, c, za, 0, jnp.where(end, 2, 3))

            if b == 0:
                @pl.when(mid)
                def _():
                    send_tok(z, b, c, zb, 1, 3)

    def prep(q, b, s=None):
        s = order[q] if s is None else s
        ids0, ids1, wt0, wt1 = [
            jnp.concatenate([met[s, b, 2 * i : 2 * i + 1], met[s, b, 2 * i + 1 : 2 * i + 2]], axis=1)
            for i in range(4)
        ]
        row = lax.broadcasted_iota(jnp.int32, (rows, tokens), 0)
        e_row = (z * side + row // cap).astype(jnp.float32)
        s_row = lax.rem(row, cap).astype(jnp.float32)
        hit0 = (ids0 == e_row).astype(jnp.float32)
        hit1 = (ids1 == e_row).astype(jnp.float32)
        hit = hit0 + hit1
        before = (
            lax.broadcasted_iota(jnp.int32, (tokens, tokens), 0)
            < lax.broadcasted_iota(jnp.int32, (tokens, tokens), 1)
        ).astype(jnp.float32).astype(jnp.bfloat16)
        count = jnp.dot(hit.astype(jnp.bfloat16), before, preferred_element_type=jnp.float32)
        pick = jnp.where(count == s_row, hit, 0.0)
        sel[q, b] = pick.astype(jnp.bfloat16)
        w = (pick * (hit0 * wt0 + hit1 * wt1)).T
        high = w.astype(jnp.bfloat16)
        mix[q, b, 0] = high
        mix[q, b, 1] = (w - high.astype(jnp.float32)).astype(jnp.bfloat16)

    def disp(q, b, c, s=None):
        s = order[q] if s is None else s
        y = jnp.dot(sel[q, b], tok[s, b, :, cols(c)], preferred_element_type=jnp.float32)
        snd[q, b, :, cols(c)] = y.astype(jnp.bfloat16)
        xin[q, b, core, band(p), cols(c)] = snd[q, b, band(p), cols(c)]
        for j in range(1, side):
            o = peer(j)
            remote(
                snd.at[q, b, band(o), cols(c)], xin.at[q, b, core, band(p), cols(c)],
                s_xs, s_x.at[q, b, c], {"ep": z * side + o},
            )

    def others(ref):
        return ref.at[pl.ds(0, (side - 1) * cap)]

    def swap_x(q, b):
        @pl.loop(0, k)
        def _(c):
            at = xin.at[q, b, core, :, cols(c)]
            landed(others(at), s_x.at[q, b, c])
            remote(at, at, s_xds, s_xd.at[q, b], partner)

    tile = min(256, half)

    def gate(q, b):
        landed(xin.at[q, b, other], s_xd.at[q, b])

        @pl.loop(0, half // tile)
        def _(i):
            at = part(i, tile)
            lo, hi = xin[q, b, 0], xin[q, b, 1]
            g = jnp.dot(lo, wg[:span, at], preferred_element_type=jnp.float32)
            g = g + jnp.dot(hi, wg[span:, at], preferred_element_type=jnp.float32)
            u = jnp.dot(lo, wu[:span, at], preferred_element_type=jnp.float32)
            u = u + jnp.dot(hi, wu[span:, at], preferred_element_type=jnp.float32)
            v = g / (1.0 + jnp.exp(-g)) * u
            hid[q, b, core, :, at] = v.astype(jnp.bfloat16)
            done = hid.at[q, b, core, :, at]
            remote(done, done, s_hs, s_h.at[q, b], partner)

    def down(q, b, c):
        @pl.when(c == 0)
        def _():
            landed(hid.at[q, b, other], s_h.at[q, b])

        y = jnp.dot(hid[q, b, 0], wd[:half, cols(c)], preferred_element_type=jnp.float32)
        y = y + jnp.dot(hid[q, b, 1], wd[half:, cols(c)], preferred_element_type=jnp.float32)
        res[q, b, :, cols(c)] = y.astype(jnp.bfloat16)
        yours = isinstance(q, int) and q == 0
        slot = core if yours else b
        at = ret.at[q, slot, band(p), cols(c)]

        def keep():
            ret[q, slot, band(p), cols(c)] = res[q, b, band(p), cols(c)]

        if yours:
            pl.when(core == b)(keep)

            @pl.when(core != b)
            def _():
                remote(res.at[q, b, band(p), cols(c)], at, s_rd, s_r.at[q, slot, c], partner)
        else:
            keep()
        for j in range(1, side):
            o = peer(j)
            where = {"ep": z * side + o, "tp": b} if yours else {"ep": z * side + o}
            remote(res.at[q, b, band(o), cols(c)], at, s_rs, s_r.at[q, slot, c], where)

    def downs(q, b):
        pl.loop(0, k)(lambda c: down(q, b, c))

    def mixed(q, b, r):
        return jnp.dot(mix[q, b, 0], r, preferred_element_type=jnp.float32) + jnp.dot(
            mix[q, b, 1], r, preferred_element_type=jnp.float32
        )

    def combine(q, b, c, t, to, add):
        landed(others(ret.at[q, b, :, cols(c)]), s_r.at[q, b, c])
        y = mixed(q, b, ret[q, b, :, cols(c)])
        if add:
            landed(racc.at[q - 1, b, c], s_p.at[q - 1, b, c])
            y = y + racc[q - 1, b, c].astype(jnp.float32)
        psend[q - 1, b, c] = y.astype(jnp.bfloat16)
        theirs = to == t

        @pl.when(theirs)
        def _():
            way = jnp.where(end, 1, 0)
            remote(
                psend.at[q - 1, b, c], home.at[way, core, c], s_ps, s_home.at[way, core, c],
                {"ep": to * side + p, "tp": b},
            )

        @pl.when(jnp.logical_not(theirs))
        def _():
            slot = jnp.where(end, jnp.where(q == 1, 0, 2), 1)
            remote(
                psend.at[q - 1, b, c], racc.at[slot, b, c], s_ps, s_p.at[slot, b, c], plane(to)
            )

    def weights():
        for i, (a, b) in enumerate(loads):
            pltpu.make_async_copy(a, b, s_wl.at[i]).wait()
        landed(wd.at[part(other, half)], s_wr)

    def own_met(b):
        send_met(z, b, za, 0)

        @pl.when(mid)
        def _():
            send_met(z, b, zb, 1)

    @pl.when(core == 0)
    def _():
        own_met(0)
        own_tok(0, 0, k)

    @pl.when(core == 1)
    def _():
        prep(0, 1)
        disp(0, 1, 0)
        got_met(z, 0)
        own_met(0)

        for h in range(2):
            at = part(h, tokens // 2)
            landed(oth.at[at], s_lent.at[h])
            for c in range(1):
                send_part(at, c, za, 0, jnp.where(end, 2, 3))

                @pl.when(mid)
                def _():
                    send_part(at, c, zb, 1, 3)

        own_tok(0, 1, k)

    prep(0, 0)
    pl.loop(0, k)(lambda c: disp(0, 0, c))
    remote(dw.at[0, :, part(other, span)], wd.at[mine], s_ws, s_wr, partner)

    @pl.when(core == 0)
    def _():
        got_met(z, 1)
        lent()
        prep(0, 1)

    own_met(1)
    def spare(c):
        @pl.when((core == 0) | (c > 0))
        def _():
            disp(0, 1, c)

    pl.when(end)(lambda: own_tok(1, 0, k))

    @pl.when(mid)
    def _():
        def relay(q, b, c):
            s = order[q]
            arrived(q, s, b, c)
            send_tok(s, b, c, za if q == 2 else zb, 0 if q == 2 else 1, 2 if q == 3 else 1)

        def learn(q, b):
            got_met(order[q], b)
            send_met(order[q], b, za if q == 2 else zb, 0 if q == 2 else 1)
            prep(q, b)

        def fold(q, b, c):
            combine(q, b, c, order[q], zb if q == 2 else za, True)

        def folds(q, b, lo, hi):
            pl.loop(lo, hi)(lambda c: fold(q, b, c))

        learn(3, 0)
        learn(2, 0)

        @pl.loop(0, k)
        def _(c):
            relay(3, 0, c)
            relay(2, 0, c)
            disp(3, 0, c)
            spare(c)

        learn(1, 0)
        learn(2, 1)

        @pl.loop(0, k)
        def _(c):
            relay(1, 0, c)
            relay(2, 1, c)
            disp(1, 0, c)
            disp(2, 0, c)

            @pl.when(c == 0)
            def _():
                weights()
                swap_x(0, 0)

            @pl.when(c == 1)
            def _():
                swap_x(3, 0)
                gate(0, 0)

            @pl.when(c == 2)
            def _():
                gate(3, 0)

        pl.loop(0, k)(lambda c: send_tok(z, 1, c, za, 0, 3))
        learn(1, 1)

        @pl.loop(0, k)
        def _(c):
            relay(1, 1, c)
            disp(1, 1, c)
            down(3, 0, c)

            @pl.when(c == 1)
            def _():
                swap_x(0, 1)
                swap_x(1, 0)

            @pl.when(c == 2)
            def _():
                gate(1, 0)

        learn(3, 1)
        gate(0, 1)

        @pl.loop(0, k)
        def _(c):
            relay(3, 1, c)
            disp(3, 1, c)
            down(1, 0, c)

            @pl.when(c == 0)
            def _():
                swap_x(2, 0)

            @pl.when(c == 1)
            def _():
                swap_x(1, 1)
                gate(2, 0)

            @pl.when(c == 2)
            def _():
                gate(1, 1)

        pl.loop(0, k)(lambda c: send_tok(z, 1, c, zb, 1, 3))
        pl.loop(0, k)(lambda c: disp(2, 1, c))
        folds(3, 0, 0, k)
        downs(1, 1)
        folds(1, 0, 0, k // 2)
        swap_x(3, 1)
        downs(2, 0)
        folds(1, 0, k // 2, k)
        swap_x(2, 1)
        gate(3, 1)
        downs(3, 1)
        gate(2, 1)

        @pl.loop(0, k // 2)
        def _(c):
            fold(1, 1, c)
            fold(2, 0, c)

        downs(2, 1)

        @pl.loop(k // 2, k)
        def _(c):
            fold(1, 1, c)
            fold(2, 0, c)

        downs(0, 0)

        @pl.loop(0, k // 2)
        def _(c):
            fold(3, 1, c)
            fold(2, 1, c)

        downs(0, 1)

        @pl.loop(k // 2, k)
        def _(c):
            fold(3, 1, c)
            fold(2, 1, c)

    @pl.when(end)
    def _():
        def take(q, b, c):
            s = z + (n - q) * step
            arrived(q, s, b, c)
            disp(q, b, c, s)

        def learn(q, b):
            s = z + (n - q) * step
            got_met(s, b)
            prep(q, b, s)

        def unit(i):
            return jnp.where(i < 3, 3 - i, i - 2), jnp.where(i < 3, 0, 1)

        def fold(q, b, c):
            combine(q, b, c, z + (n - q) * step, za, False)

        learn(3, 0)

        @pl.loop(0, k)
        def _(c):
            take(3, 0, c)

            @pl.when(c < k // 2)
            def _():
                spare(c)

            @pl.when(c == 1)
            def _():
                weights()
                swap_x(0, 0)

            @pl.when(c == 2)
            def _():
                gate(0, 0)

        quarter = k // 4

        def piece(f, q, b, j, m=1):
            pl.loop(j * quarter, (j + m) * quarter)(lambda c: f(q, b, c))

        piece(disp, 0, 1, 2, 2)
        learn(2, 0)
        swap_x(3, 0)
        piece(take, 2, 0, 0)
        gate(3, 0)
        piece(take, 2, 0, 1)
        piece(down, 3, 0, 0, 2)
        piece(take, 2, 0, 2)
        piece(take, 2, 0, 3)
        piece(down, 3, 0, 2, 2)
        piece(fold, 3, 0, 0)

        @pl.loop(1, 5)
        def _(i):
            q, b = unit(i)
            q1, b1 = unit(i + 1)
            q0, b0 = unit(i - 1)
            learn(q1, b1)
            piece(take, q1, b1, 0)
            piece(fold, q0, b0, 1)
            swap_x(q, b)
            piece(take, q1, b1, 1)
            gate(q, b)
            piece(fold, q0, b0, 2)
            piece(take, q1, b1, 2)
            piece(down, q, b, 0, 2)
            piece(fold, q0, b0, 3)
            piece(take, q1, b1, 3)
            piece(down, q, b, 2, 2)

            @pl.when(i == 1)
            def _():
                swap_x(0, 1)

            @pl.when(i == 2)
            def _():
                gate(0, 1)

            @pl.when(i == 4)
            def _():
                piece(down, 0, 1, 0, 3)

            piece(fold, q, b, 0)

        swap_x(3, 1)
        piece(fold, 2, 1, 1)
        gate(3, 1)
        piece(fold, 2, 1, 2, 2)
        downs(3, 1)
        downs(0, 0)
        piece(down, 0, 1, 3)
        piece(fold, 3, 1, 0, 4)

    def last(h, c, ways):
        at = ret.at[0, h, :, cols(c)]
        pl.when(core == h)(lambda: landed(others(at), s_r.at[0, h, c]))
        pl.when(core != h)(lambda: landed(at, s_r.at[0, h, c]))
        y = mixed(0, core, at[...])
        for way in ways:
            landed(home.at[way, h, c], s_home.at[way, h, c])
            y = y + home[way, h, c].astype(jnp.float32)
        out[:, pl.ds(pl.multiple_of(h * span + c * wide, wide), wide)] = y.astype(out.dtype)

    @pl.when(end)
    def _():
        @pl.loop(0, k)
        def _(c):
            last(0, c, [0])
            last(1, c, [0])

    @pl.when(mid)
    def _():
        @pl.loop(0, k)
        def _(c):
            last(0, c, [0, 1])
            last(1, c, [0, 1])

    drain = landed
    drain(met.at[z, core], s_os.at[0])
    drain(oth, s_os.at[1])
    drain(wd.at[mine], s_ws)
    sent = pl.ds(0, (side - 1) * cap)

    @pl.when(end)
    def _():
        drain(tok.at[0], s_toks.at[0])
        drain(met.at[0], s_mets.at[0])

    @pl.when(mid)
    def _():
        for way in range(2):
            drain(tok.at[pl.ds(0, 2 + way)], s_toks.at[way])
            drain(met.at[pl.ds(0, 2 + way)], s_mets.at[way])

    drain(snd.at[:, :, sent], s_xs)
    drain(res.at[:, :, sent], s_rs)
    drain(snd, s_xds)
    drain(hid.at[:, :, 0], s_hs)
    drain(psend, s_ps)
    drain(res.at[0, 0, pl.ds(0, cap)], s_rd)


def body(
    tokens, norm_gain, norm_bias, gate_weight, up_weight, down_weight, expert_ids, route_weights
):
    count, width = tokens.shape
    experts = lax.axis_size("ep")
    cap = max(4 * count // experts, 4)
    side = experts // LINE
    half = gate_weight.shape[2]
    rows = side * cap
    span = width // 2
    wide = span // CHUNKS
    bf = jnp.bfloat16
    dma = pltpu.SemaphoreType.DMA
    hbm = pl.BlockSpec(memory_space=pl.ANY)
    return pl.pallas_call(
        functools.partial(kernel, side),
        out_shape=pltpu.VMEM((count, width), bf),
        in_specs=[hbm] * 8,
        out_specs=pl.BlockSpec(memory_space=pltpu.VMEM),
        scratch_shapes=[
            pltpu.VMEM((count, width), bf),
            pltpu.VMEM((1, width), jnp.float32),
            pltpu.VMEM((1, width), jnp.float32),
            pltpu.VMEM((2, count), jnp.int32),
            pltpu.VMEM((2, count), jnp.float32),
            pltpu.VMEM((count, span), bf),
            pltpu.VMEM((LINE, 2, count, span), bf),
            pltpu.VMEM((LINE, 2, 8, count // 2), jnp.float32),
            pltpu.VMEM((width, half), bf),
            pltpu.VMEM((width, half), bf),
            pltpu.VMEM((2 * half, span), bf),
            pltpu.VMEM((LINE, 2, rows, count), bf),
            pltpu.VMEM((LINE, 2, 2, count, rows), bf),
            pltpu.VMEM((LINE, 2, rows, span), bf),
            pltpu.VMEM((LINE, 2, 2, rows, span), bf),
            pltpu.VMEM((LINE, 2, 2, rows, half), bf),
            pltpu.VMEM((LINE, 2, rows, span), bf),
            pltpu.VMEM((LINE, 2, rows, span), bf),
            pltpu.VMEM((LINE - 1, 2, CHUNKS, count, wide), bf),
            pltpu.VMEM((LINE - 1, 2, CHUNKS, count, wide), bf),
            pltpu.VMEM((2, 2, CHUNKS, count, wide), bf),
            dma((4 + count // min(64, count),)),
            dma((2,)),
            dma((3,)),
            dma,
            dma,
            dma((LINE - 1, 2, CHUNKS)),
            dma((2,)),
            dma((LINE, 2)),
            dma((2,)),
            dma((2,)),
            dma((LINE, 2, CHUNKS)),
            dma,
            dma((LINE, 2)),
            dma,
            dma((LINE, 2)),
            dma,
            dma((LINE, 2, CHUNKS)),
            dma,
            dma((LINE - 1, 2, CHUNKS)),
            dma,
            dma((2, 2, CHUNKS)),
            dma,
        ],
        compiler_params=pltpu.CompilerParams(
            collective_id=0, has_side_effects=True, vmem_limit_bytes=56 * 1024 * 1024
        ),
    )(
        tokens, norm_gain[None], norm_bias[None], expert_ids.T, route_weights.T,
        gate_weight, up_weight, down_weight,
    )


def solution(mesh):
    placed = (
        P(("ep", "tp"), None),
        P(),
        P(),
        P("ep", None, "tp"),
        P("ep", None, "tp"),
        P("ep", "tp", None),
        P(("ep", "tp"), None),
        P(("ep", "tp"), None),
    )
    return jax.shard_map(
        body, mesh=mesh, in_specs=placed, out_specs=P(("ep", "tp"), None), check_vma=False
    )
```
